128 devices in a mesh: rep: 16 (over z, x), fs: 4 (over y), tp: 2 (over core).
Axes of the slice: x: 4, y: 4, z: 4, core: 2. Of those that a mesh axis runs over, the one named last changes fastest.
Arguments:
- inputs: bfloat16 [16384, 2048], P(('rep', 'fs', 'tp')), may hold values from -6 to 6
- out_grad: bfloat16 [16384, 2048], P(('rep', 'fs', 'tp')), may hold values from -24 to 24
- pre_act: bfloat16 [16384, 8192], P('rep', ('fs', 'tp')), may hold values from -6 to 6
- w_up: bfloat16 [2048, 8192], P('rep', ('fs', 'tp')), may hold values from -0.125 to 0.125
- w_down_t: bfloat16 [2048, 8192], P('rep', ('fs', 'tp')), may hold values from -0.0625 to 0.0625
Outputs:
- grad_in: bfloat16 [16384, 2048], P(('rep', 'fs', 'tp'))
- grad_up: float32 [2048, 8192], P('rep', ('fs', 'tp'))
- grad_down_t: float32 [2048, 8192], P('rep', ('fs', 'tp'))
The draws below stay inside these ranges and needn't reach their ends.
All inputs are finite; a program needn't handle non-finite values.
Results may differ from the reference program's by a relative error of at most 0.014.
Values may be sent and summed in bfloat16 or wider, within the bound.
A program may use at most 128 MiB of HBM per device.

```python
import jax
import jax.numpy as jnp
from jax import lax

D = 2048
FF = 8192
TOKENS = 16384
N_FS = 4
N_TP = 2


def with_spikes(entries, rng, source, target, shards_of, factor):
    owner, partner = [(jnp.arange(entries.shape[position]) // (entries.shape[position] // shards_of)).reshape([-1 if axis == position else 1 for axis in range(entries.ndim)]) for position in (source, target)]
    chosen = jax.random.permutation(rng, shards_of)[partner]
    strong = (owner == chosen) | (owner == (partner + shards_of // 2) % shards_of)
    return jnp.where(strong, factor * entries, entries)


def shard_levels(own_key, dims, cuts, low, top_value):
    level, own = 1.0, jax.random.fold_in(own_key, 6)
    for dim, shards_of in cuts:
        draws = jnp.exp(jax.random.uniform(jax.random.fold_in(own, dim), (shards_of,), jnp.float32, low / len(cuts), top_value / len(cuts)))
        level = level * jnp.repeat(draws, dims[dim] // shards_of).reshape([-1 if axis == dim else 1 for axis in range(len(dims))])
    return level


def noise(rng, extent, scale, most, cuts=(), dtype=jnp.bfloat16):
    factor_of = shard_levels(rng, extent, cuts, -0.22, 0.18) if cuts else 1.0
    values = jax.random.normal(rng, extent, jnp.float32) * scale * factor_of
    return jnp.minimum(jnp.maximum(values, -most), most).astype(dtype)


def noise_with(own_key, dims, spread, reach, pieces, heavy, kind=jnp.bfloat16):
    result = spread * jax.random.normal(own_key, dims, jnp.float32)
    if pieces:
        result = result * shard_levels(own_key, dims, pieces, -0.22, 0.18)
    return jnp.clip(with_spikes(result, jax.random.fold_in(own_key, 3), *heavy), -reach, reach).astype(kind)


def setup_inputs(seed: int = 0) -> dict:
    arg_keys = jax.random.split(jax.random.key(seed), 6)
    inputs = noise(arg_keys[0], (TOKENS, D), 1.0, 6.0, ((0, 128),))
    out_grad = noise_with(arg_keys[1], (TOKENS, D), 1.0, 24.0, ((0, 128),), (0, 1, 128, 5.5))
    pre_act = noise(arg_keys[2], (TOKENS, FF), 1.0, 6.0, ((0, 16), (1, 8)))
    w_up = noise(arg_keys[3], (D, FF), D ** -0.5, 0.125, ((0, 16), (1, 8)))
    w_down_t = noise(arg_keys[4], (D, FF), FF ** -0.5, 0.0625, ((0, 16), (1, 8)))
    return {"inputs": inputs, "out_grad": out_grad, "pre_act": pre_act, "w_up": w_up, "w_down_t": w_down_t}


def reference(inputs, out_grad, pre_act, w_up, w_down_t):
    pre_float = pre_act.astype(jnp.float32)
    linear = jnp.maximum(pre_float, 0.0)
    squared = (linear * linear).astype(jnp.bfloat16)
    grad_squared = jnp.dot(out_grad, w_down_t, preferred_element_type=jnp.float32)
    grad_pre = (grad_squared * 2.0 * linear).astype(jnp.bfloat16)
    factor = float(TOKENS) ** -0.5
    grad_down_t = jnp.dot(out_grad.T, squared, preferred_element_type=jnp.float32) * factor
    grad_up = jnp.dot(inputs.T, grad_pre, preferred_element_type=jnp.float32) * factor
    blocks = N_FS * N_TP
    width = FF // blocks
    total = jnp.zeros((inputs.shape[0], D), jnp.float32)
    for index in range(blocks):
        term = jnp.dot(grad_pre[:, index * width:(index + 1) * width], w_up[:, index * width:(index + 1) * width].T, preferred_element_type=jnp.float32)
        term = lax.optimization_barrier(term.astype(jnp.bfloat16))
        total = total + term.astype(jnp.float32)
    return total.astype(jnp.bfloat16), grad_up, grad_down_t
```

```python
import jax
import jax.numpy as jnp
from jax import lax
from jax.experimental import pallas as pl
from jax.experimental.pallas import tpu as pltpu
from jax.sharding import PartitionSpec as P

MESH = pl.DeviceIdType.MESH
BF16, F32 = jnp.bfloat16, jnp.float32
STEP = {"zp": (1, 0), "zm": (-1, 0), "xp": (0, 1), "xm": (0, -1)}
PLUS = ((0, 2), (1, 3))
TURN = (1, -1)
SEMS = 160


def kernel(
    inp, og, pre_in, wu_in, wd_in, gi_out, gu_out, gd_out,
    tok_g, tok_x, w_d, w_u, pre, sq, gp, turned, part_d, part_u, part_i,
    fwd1, lft1, rgt1, sum1, fwd2, lft2, rgt2,
    pair_in, hop_f, hop_l, hop_r, res_i, res_w, send_sem, recv_sem, local_sem,
):
    rep, fs, tp = lax.axis_index("rep"), lax.axis_index("fs"), lax.axis_index("tp")
    z, x = lax.div(rep, 4), lax.rem(rep, 4)
    tokens, weights, parts = (tok_g, tok_x), (w_d, w_u), (part_d, part_u)
    factor = 1.0 / 128.0

    def ring(v, d):
        return lax.rem(v + d % 4, 4)

    target = {
        "zp": {"rep": ring(z, 1) * 4 + x},
        "zm": {"rep": ring(z, -1) * 4 + x},
        "xp": {"rep": z * 4 + ring(x, 1)},
        "xm": {"rep": z * 4 + ring(x, -1)},
        "yp": {"fs": ring(fs, 1)},
        "ym": {"fs": ring(fs, -1)},
        "co": {"tp": 1 - tp},
    }
    ids, started = {}, []

    def remote(to, src, dst, key):
        n = ids.setdefault(key, len(ids))
        return pltpu.make_async_remote_copy(
            src_ref=src, dst_ref=dst, send_sem=send_sem.at[n], recv_sem=recv_sem.at[n],
            device_id=target[to], device_id_type=MESH,
        )

    def send(to, src, dst, key):
        copy = remote(to, src, dst, key)
        copy.start()
        started.append(copy)

    def got(dst, key):
        remote("co", dst, dst, key).wait_recv()

    def rows(start, size):
        return pl.ds(pl.multiple_of(start, size), size)

    def add(dst, *srcs, size=32, scale=None):
        def one(i, carry):
            r = rows(i * size, size)
            total = srcs[0][r, :].astype(F32)
            for src in srcs[1:]:
                total = total + src[r, :].astype(F32)
            if scale is not None:
                total = total * scale
            dst[r, :] = total.astype(dst.dtype)
            return carry

        lax.fori_loop(0, dst.shape[0] // size, one, 0)

    def tok(a, df, mine, h):
        core = tp if mine else 1 - tp
        return tokens[a].at[rows((ring(fs, df) * 2 + core) * 128 + h * 64, 64), :]

    def tok_y(a, df, h, s):
        p = tok(a, df, True, h)
        send("yp" if s > 0 else "ym", p, p, ("t", a, (df - s) % 4, True, h))

    def tok_co(a, df, h):
        p = tok(a, df, True, h)
        send("co", p, p, ("t", a, df % 4, False, h))

    def tok_got(a, df, mine, h):
        got(tok(a, df, mine, h), ("t", a, df % 4, mine, h))

    def tok_own(a):
        tok_y(a, 0, 0, 1)
        tok_y(a, 0, 1, -1)
        tok_y(a, 0, 1, 1)
        tok_y(a, 0, 0, -1)
        tok_co(a, 0, 0)
        tok_co(a, 0, 1)

    def tok_first(a):
        for df, h in ((-1, 0), (1, 1)):
            tok_got(a, df, True, h)
            tok_y(a, df, h, -df)
            tok_co(a, df, h)

    def tok_second(a):
        for df, h in ((-1, 1), (1, 0)):
            tok_got(a, df, True, h)
            tok_co(a, df, h)

    def tok_third(a):
        for h in (0, 1):
            tok_got(a, 2, True, h)
            tok_co(a, 2, h)

    def tok_partner(a):
        for df in (0, -1, 1, 2):
            for h in (0, 1):
                tok_got(a, df, False, h)

    def chunk(dz, dx):
        return (ring(z, dz) * 4 + ring(x, dx)) * 128

    def offs(half, d1, d2):
        return (d1, d2) if half == 0 else (d2, d1)

    def way(half, second, s):
        return ("zx"[half ^ second]) + ("p" if s > 0 else "m")

    def w_piece(w, half, d1, d2):
        dz, dx = offs(half, d1, d2)
        return weights[w].at[rows(chunk(dz, dx) + half * 64, 64), :]

    def w_send(w, half, d1, d2, second, s):
        p = w_piece(w, half, d1, d2)
        e1, e2 = (0, s) if second else (s, 0)
        send(way(half, second, s), p, p, ("w", w, half, (d1 - e1) % 4, (d2 - e2) % 4))

    def w_got(w, half, d1, d2):
        got(w_piece(w, half, d1, d2), ("w", w, half, d1 % 4, d2 % 4))

    def w_own(w):
        for second in (0, 1):
            for half in (0, 1):
                for s in (1, -1):
                    w_send(w, half, 0, 0, second, s)

    def w_first(w):
        for s in (TURN[w], -TURN[w]):
            for half in (0, 1):
                w_got(w, half, -s, 0)
                if s == TURN[w]:
                    w_send(w, half, -s, 0, 0, s)
                for e in (1, -1):
                    w_send(w, half, -s, 0, 1, e)

    def w_second(w):
        for half in (0, 1):
            w_got(w, half, 2, 0)
            for e in (1, -1):
                w_send(w, half, 2, 0, 1, e)

    def w_third(w, d1s):
        for d1 in d1s:
            for half in (0, 1):
                for s in (1, -1):
                    w_got(w, half, d1, -s)
                    if s == (1 if d1 in PLUS[w] else -1):
                        w_send(w, half, d1, -s, 1, s)

    def w_last(w):
        for d1 in (0, 1, 3, 2):
            for half in (0, 1):
                w_got(w, half, d1, 2)

    def unit(w, half, da, db):
        dz, dx = (db, da) if half == 0 else (da, db)
        return parts[w].at[rows(chunk(dz, dx), 128), half * 512 : half * 512 + 512]

    def rs_way(half, second, s):
        return way(1 - half, second, s)

    def sign(w, db):
        return 1 if db % 4 in PLUS[w] else -1

    def end1(s):
        return (lft1, "l1") if s > 0 else (rgt1, "r1")

    def end2(s):
        return (lft2, "l2") if s > 0 else (rgt2, "r2")

    def rs_far(w, half, db):
        db = db % 4
        send(rs_way(half, 0, sign(w, db)), unit(w, half, 2, db), fwd1.at[w, half, db], ("f1", w, half, db))

    def rs_near(w, half, db):
        db, s = db % 4, -sign(w, db)
        buf, name = end1(s)
        send(rs_way(half, 0, s), unit(w, half, s, db), buf.at[w, half, db], (name, w, half, db))

    def rs_relay(w, half, db):
        db, s = db % 4, sign(w, db)
        got(fwd1.at[w, half, db], ("f1", w, half, db))
        mine = unit(w, half, s, db)
        add(mine, mine, fwd1.at[w, half, db])
        buf, name = end1(s)
        send(rs_way(half, 0, s), mine, buf.at[w, half, db], (name, w, half, db))

    def rs_mid(w, half, db):
        db, s = db % 4, TURN[w]
        for e in (1, -1):
            buf, name = end1(e)
            got(buf.at[w, half, db], (name, w, half, db))
        terms = [unit(w, half, 0, db), lft1.at[w, half, db], rgt1.at[w, half, db]]
        mine = sum1.at[w, half, db]
        if db == 2:
            add(mine, *terms)
            send(rs_way(half, 1, s), mine, fwd2.at[w, half], ("f2", w, half))
        elif db == -s % 4:
            add(mine, *terms)
            buf, name = end2(-s)
            send(rs_way(half, 1, -s), mine, buf.at[w, half], (name, w, half))
        elif db == s % 4:
            got(fwd2.at[w, half], ("f2", w, half))
            add(mine, *terms, fwd2.at[w, half])
            buf, name = end2(s)
            send(rs_way(half, 1, s), mine, buf.at[w, half], (name, w, half))
        else:
            for e in (1, -1):
                buf, name = end2(e)
                got(buf.at[w, half], (name, w, half))
            add(
                res_w.at[w, :, half * 512 : half * 512 + 512],
                *terms, lft2.at[w, half], rgt2.at[w, half], scale=factor,
            )

    def rs_start(w, dz):
        if dz == 2:
            rs_far(w, 0, 2)
            for db in (2, 1, 3, 0):
                rs_far(w, 1, db)
            rs_near(w, 0, 2)
        else:
            rs_far(w, 0, dz)
            rs_near(w, 0, dz)
            if dz != 0:
                for db in (2, 1, 3, 0):
                    if (1 if dz == 1 else -1) == -sign(w, db):
                        rs_near(w, 1, db)

    def block(df, mine):
        core = tp if mine else 1 - tp
        return (ring(fs, df) * 2 + core) * 128

    def gi_rows(df, h):
        return part_i.at[rows(block(df, True) + h * 64, 64), :]

    def gi_pair():
        for df in (2, 1, 3, 0):
            src = part_i.at[rows(block(df, False), 128), :]
            send("co", src, pair_in.at[df], ("pi", df))

    def gi_sum(df):
        got(pair_in.at[df], ("pi", df))
        mine = part_i.at[rows(block(df, True), 128), :]
        if df != 0:
            add(mine, mine, pair_in.at[df], size=16)

    def gi_far():
        gi_sum(2)
        send("yp", gi_rows(2, 0), hop_f.at[0], ("gf", 0))
        send("ym", gi_rows(2, 1), hop_f.at[1], ("gf", 1))
        gi_sum(1)
        send("yp", gi_rows(1, 1), hop_l.at[1], ("gl", 1))
        gi_sum(3)
        send("ym", gi_rows(3, 0), hop_r.at[0], ("gr", 0))
        gi_sum(0)

    def gi_relay():
        got(hop_f.at[0], ("gf", 0))
        add(gi_rows(1, 0), gi_rows(1, 0), hop_f.at[0], size=16)
        send("yp", gi_rows(1, 0), hop_l.at[0], ("gl", 0))
        got(hop_f.at[1], ("gf", 1))
        add(gi_rows(3, 1), gi_rows(3, 1), hop_f.at[1], size=16)
        send("ym", gi_rows(3, 1), hop_r.at[1], ("gr", 1))

    def gi_end():
        for h in (0, 1):
            got(hop_l.at[h], ("gl", h))
            got(hop_r.at[h], ("gr", h))
            add(
                res_i.at[pl.ds(h * 64, 64), :],
                gi_rows(0, h), pair_in.at[0, pl.ds(h * 64, 64), :], hop_l.at[h], hop_r.at[h], size=16,
            )

    def squares():
        def one(i, carry):
            r = rows(i * 32, 32)
            linear = jnp.maximum(pre[r, :].astype(F32), 0.0)
            sq[r, :] = (linear * linear).astype(BF16)
            return carry

        lax.fori_loop(0, 32, one, 0)

    def grad_tile(w, dz):
        right = (sq, gp)[w]
        start = ring(z, dz) * 512
        turned[...] = tokens[w][:, rows(start, 512)].T

        def one(j, carry):
            c = rows(j * 512, 512)
            parts[w][rows(start, 512), c] = jnp.dot(
                turned[...], right[:, c], preferred_element_type=F32
            ).astype(BF16)
            return carry

        lax.fori_loop(0, 2, one, 0)

    def pre_tile(i):
        def one(j, carry):
            r, c = rows(i * 512, 512), rows(j * 256, 256)
            acc = jnp.dot(tok_g[r, :], w_d[:, c], preferred_element_type=F32)
            linear = jnp.maximum(pre[r, c].astype(F32), 0.0)
            gp[r, c] = (acc * 2.0 * linear).astype(BF16)
            return carry

        lax.fori_loop(0, 4, one, 0)

    def term_tile(i):
        def one(j, carry):
            r, c = rows(i * 512, 512), rows(j * 512, 512)
            part_i[r, c] = lax.dot_general(
                gp[r, :], w_u[c, :], (((1,), (1,)), ((), ())), preferred_element_type=F32
            ).astype(BF16)
            return carry

        lax.fori_loop(0, 4, one, 0)

    own = rows((fs * 2 + tp) * 128, 128)
    mine = rows(rep * 128, 128)
    local = [
        pltpu.make_async_copy(src, dst, local_sem.at[n])
        for n, (src, dst) in enumerate(
            (
                (wd_in, w_d.at[mine, :]),
                (og, tok_g.at[own, :]),
                (wu_in, w_u.at[mine, :]),
                (inp, tok_x.at[own, :]),
                (pre_in, pre),
            )
        )
    ]
    for copy in local:
        copy.start()
    barrier = pltpu.get_barrier_semaphore()
    for to in target.values():
        pl.semaphore_signal(barrier, inc=1, device_id=to, device_id_type=MESH)
    pl.semaphore_wait(barrier, len(target))

    local[0].wait()
    w_own(0)
    local[1].wait()
    tok_own(0)
    local[2].wait()
    local[3].wait()
    local[4].wait()
    squares()
    w_first(0)
    tok_first(0)
    tok_own(1)
    w_third(0, (0,))
    w_second(0)
    w_own(1)
    tok_second(0)
    w_third(0, (1, 3))
    w_first(1)
    tok_third(0)
    tok_partner(0)
    grad_tile(0, 2)
    rs_start(0, 2)
    w_third(0, (2,))
    grad_tile(0, 1)
    rs_start(0, 1)
    w_second(1)
    tok_first(1)
    grad_tile(0, 3)
    rs_start(0, 3)
    w_third(1, (0,))
    grad_tile(0, 0)
    rs_start(0, 0)
    w_last(0)
    pre_tile(0)
    w_third(1, (1, 3))
    tok_second(1)
    pre_tile(1)
    w_third(1, (2,))
    tok_third(1)
    tok_partner(1)
    grad_tile(1, 2)
    rs_start(1, 2)
    grad_tile(1, 1)
    rs_start(1, 1)
    grad_tile(1, 3)
    rs_start(1, 3)
    grad_tile(1, 0)
    rs_start(1, 0)
    w_last(1)
    term_tile(0)
    for db in (2, 1):
        for half in (0, 1):
            rs_relay(0, half, db)
    term_tile(1)
    gi_pair()
    for db in (3, 0):
        for half in (0, 1):
            rs_relay(0, half, db)
    gi_far()
    for w in (0, 1):
        order = (2, -TURN[w], TURN[w], 0)
        if w == 0:
            for db in (2, 1, 3, 0):
                for half in (0, 1):
                    rs_mid(0, half, order[0]) if db == 2 else None
                    rs_relay(1, half, db)
            gi_relay()
            for db in order[1:]:
                for half in (0, 1):
                    rs_mid(0, half, db)
        else:
            gi_end()
            for db in order:
                for half in (0, 1):
                    rs_mid(1, half, db)
    outs = [
        pltpu.make_async_copy(src, dst, local_sem.at[n])
        for n, (src, dst) in enumerate(((res_i, gi_out), (res_w.at[1], gu_out), (res_w.at[0], gd_out)))
    ]
    for copy in outs:
        copy.start()
    for copy in started:
        copy.wait_send()
    for copy in outs:
        copy.wait()


def on_device(inputs, out_grad, pre_act, w_up, w_down_t):
    anywhere = pl.BlockSpec(memory_space=pl.ANY)

    def vm(*shape, kind=BF16):
        return pltpu.VMEM(shape, kind)

    return pl.pallas_call(
        kernel,
        out_shape=(
            jax.ShapeDtypeStruct((128, 2048), BF16),
            jax.ShapeDtypeStruct((128, 1024), F32),
            jax.ShapeDtypeStruct((128, 1024), F32),
        ),
        in_specs=[anywhere] * 5,
        out_specs=(anywhere,) * 3,
        scratch_shapes=[
            vm(1024, 2048), vm(1024, 2048), vm(2048, 1024), vm(2048, 1024),
            vm(1024, 1024), vm(1024, 1024), vm(1024, 1024), vm(512, 1024),
            vm(2048, 1024), vm(2048, 1024), vm(1024, 2048),
            vm(2, 2, 4, 128, 512), vm(2, 2, 4, 128, 512), vm(2, 2, 4, 128, 512), vm(2, 2, 4, 128, 512),
            vm(2, 2, 128, 512), vm(2, 2, 128, 512), vm(2, 2, 128, 512),
            vm(4, 128, 2048), vm(2, 64, 2048), vm(2, 64, 2048), vm(2, 64, 2048),
            vm(128, 2048), vm(2, 128, 1024, kind=F32),
            pltpu.SemaphoreType.DMA((SEMS,)), pltpu.SemaphoreType.DMA((SEMS,)), pltpu.SemaphoreType.DMA((8,)),
        ],
        compiler_params=pltpu.CompilerParams(
            collective_id=0, has_side_effects=True, vmem_limit_bytes=67_000_000
        ),
        name="backward",
    )(inputs, out_grad, pre_act, w_up, w_down_t)


def solution(mesh):
    rows_all = P(("rep", "fs", "tp"), None)
    tiles = P("rep", ("fs", "tp"))
    return jax.shard_map(
        on_device,
        mesh=mesh,
        in_specs=(rows_all, rows_all, tiles, tiles, tiles),
        out_specs=(rows_all, tiles, tiles),
        check_vma=False,
    )
```

```python
import jax
import jax.numpy as jnp
from jax import lax
from jax.experimental import pallas as pl
from jax.experimental.pallas import tpu as pltpu
from jax.sharding import PartitionSpec as P

MESH = pl.DeviceIdType.MESH
BF16, F32 = jnp.bfloat16, jnp.float32
STEP = {"zp": (1, 0), "zm": (-1, 0), "xp": (0, 1), "xm": (0, -1)}
PLUS = ((0, 2), (1, 3))
TURN = (1, -1)
PLAN = (
    ("begin",), ("squares",), ("w_own", 1), ("tok_first", 0), ("w_first", 0, 1), ("w_first", 0, -1),
    ("w_first", 1, -1), ("tok_own", 1), ("tok_third", 0), ("w_second", 0), ("tok_second", 0), ("w_second", 1),
    ("w_third", 0, 3), ("tok_partner", 0), ("w_third", 0, 0), ("grad_tile", 0, 2), ("w_third", 0, 1),
    ("tok_first", 1), ("w_first", 1, 1), ("w_third", 1, 2), ("w_third", 0, 2), ("grad_tile", 0, 1),
    ("rs_far", 0, 2), ("grad_tile", 0, 0), ("rs_near", 0, 1), ("grad_tile", 0, 3), ("rs_far", 0, 3),
    ("w_third", 1, 0), ("w_last", 0), ("w_third", 1, 1), ("w_third", 1, 3), ("pre_tile", 1, 1),
    ("tok_second", 1), ("pre_tile", 0, 0), ("pre_tile", 0, 1), ("rs_near", 0, 0), ("tok_third", 1),
    ("rs_relay", 0, 2), ("tok_partner", 1), ("pre_tile", 1, 0), ("rs_near", 0, 2), ("rs_far", 0, 0),
    ("grad_tile", 1, 2), ("rs_far", 0, 1), ("rs_far", 1, 2), ("grad_tile", 1, 1), ("grad_tile", 1, 3),
    ("rs_relay", 0, 3), ("rs_far", 1, 1), ("rs_near", 1, 1), ("w_last", 1), ("rs_far", 1, 3),
    ("term_tile", 0, 1), ("grad_tile", 1, 0), ("term_tile", 0, 0), ("rs_near", 0, 3), ("term_tile", 1, 1),
    ("rs_near", 1, 0), ("rs_relay", 1, 2), ("rs_near", 1, 2), ("rs_far", 1, 0), ("term_tile", 1, 0),
    ("rs_mid", 0, 2), ("gi_pair",), ("rs_relay", 0, 1), ("rs_relay", 1, 3), ("rs_relay", 1, 1),
    ("rs_relay", 0, 0), ("gi_far",), ("rs_near", 1, 3), ("rs_mid", 1, 2), ("rs_mid", 0, 3), ("gi_relay",),
    ("rs_mid", 0, 1), ("rs_relay", 1, 0), ("rs_mid", 1, 3), ("rs_mid", 1, 1), ("rs_mid", 0, 0), ("gi_end",),
    ("rs_mid", 1, 0), ("finish",),
)


def kernel(
    inp, og, pre_in, wu_in, wd_in, gi_out, gu_out, gd_out,
    tok_g, tok_x, w_d, w_u, pre, sq, gp, turned, part_d, part_u, part_i,
    fwd1, lft1, rgt1, sum1, fwd2, lft2, rgt2,
    pair_in, hop_f, hop_l, hop_r, send_sem, recv_sem, local_sem,
):
    rep, fs, tp = lax.axis_index("rep"), lax.axis_index("fs"), lax.axis_index("tp")
    z, x = lax.div(rep, 4), lax.rem(rep, 4)
    tokens, weights, parts = (tok_g, tok_x), (w_d, w_u), (part_d, part_u)
    factor = 1.0 / 128.0

    def ring(v, d):
        return lax.rem(v + d % 4, 4)

    target = {
        "zp": {"rep": ring(z, 1) * 4 + x},
        "zm": {"rep": ring(z, -1) * 4 + x},
        "xp": {"rep": z * 4 + ring(x, 1)},
        "xm": {"rep": z * 4 + ring(x, -1)},
        "yp": {"fs": ring(fs, 1)},
        "ym": {"fs": ring(fs, -1)},
        "co": {"tp": 1 - tp},
    }
    groups, classes = {}, {}

    def remote(to, src, dst, group, kind):
        k = classes.setdefault(kind, len(classes))
        n = groups.setdefault(group, len(groups))
        return pltpu.make_async_remote_copy(
            src_ref=src, dst_ref=dst, send_sem=send_sem.at[k], recv_sem=recv_sem.at[n],
            device_id=target[to], device_id_type=MESH,
        )

    def send(to, src, dst, group):
        remote(to, src, dst, group, (group[0], *group[1:2])).start()

    def got(like, group):
        remote("co", like, like, group, (group[0], *group[1:2])).wait_recv()

    def sent(like, kind):
        remote("co", like, like, (), kind).wait_send()

    def rows(start, size):
        return pl.ds(pl.multiple_of(start, size), size)

    def add(dst, *srcs, size=32, scale=None):
        def one(i, carry):
            r = rows(i * size, size)
            total = srcs[0][r, :].astype(F32)
            for src in srcs[1:]:
                total = total + src[r, :].astype(F32)
            if scale is not None:
                total = total * scale
            dst[r, :] = total.astype(dst.dtype)
            return carry

        lax.fori_loop(0, dst.shape[0] // size, one, 0)

    def tok(a, df, mine, h):
        core = tp if mine else 1 - tp
        return tokens[a].at[rows((ring(fs, df) * 2 + core) * 128 + h * 64, 64), :]

    def tok_y(a, df, h, s, stage):
        p = tok(a, df, True, h)
        send("yp" if s > 0 else "ym", p, p, ("tok", a, stage))

    def tok_co(a, df, h):
        p = tok(a, df, True, h)
        send("co", p, p, ("tok", a, "partner"))

    def tok_got(a, pieces, stage):
        got(tokens[a].at[0 : 64 * pieces, :], ("tok", a, stage))

    def tok_own(a):
        tok_y(a, 0, 0, 1, 1)
        tok_y(a, 0, 1, -1, 1)
        tok_y(a, 0, 1, 1, 2)
        tok_y(a, 0, 0, -1, 2)
        tok_co(a, 0, 0)
        tok_co(a, 0, 1)

    def tok_first(a):
        tok_got(a, 2, 1)
        for df, h in ((-1, 0), (1, 1)):
            tok_y(a, df, h, -df, 3)
            tok_co(a, df, h)

    def tok_second(a):
        tok_got(a, 2, 2)
        for df, h in ((-1, 1), (1, 0)):
            tok_co(a, df, h)

    def tok_third(a):
        tok_got(a, 2, 3)
        for h in (0, 1):
            tok_co(a, 2, h)

    def tok_partner(a):
        tok_got(a, 8, "partner")

    def chunk(dz, dx):
        return (ring(z, dz) * 4 + ring(x, dx)) * 128

    def offs(half, d1, d2):
        return (d1, d2) if half == 0 else (d2, d1)

    def way(half, second, s):
        return ("zx"[half ^ second]) + ("p" if s > 0 else "m")

    def w_piece(w, half, d1, d2):
        dz, dx = offs(half, d1, d2)
        return weights[w].at[rows(chunk(dz, dx) + half * 64, 64), :]

    def w_send(w, half, d1, d2, second, s, stage):
        p = w_piece(w, half, d1, d2)
        send(way(half, second, s), p, p, ("w", w, *stage))

    def w_got(w, pieces, stage):
        got(weights[w].at[0 : 64 * pieces, :], ("w", w, *stage))

    def w_own(w):
        for second in (0, 1):
            for half in (0, 1):
                for s in (1, -1):
                    w_send(w, half, 0, 0, second, s, (3, 0) if second else (1, s))

    def w_first(w, s):
        w_got(w, 2, (1, s))
        if s == TURN[w]:
            for half in (0, 1):
                w_send(w, half, -s, 0, 0, s, (2,))
        for half in (0, 1):
            for e in (1, -1):
                w_send(w, half, -s, 0, 1, e, (3, -s % 4))

    def w_second(w):
        w_got(w, 2, (2,))
        for half in (0, 1):
            for e in (1, -1):
                w_send(w, half, 2, 0, 1, e, (3, 2))

    def w_third(w, d1):
        w_got(w, 4, (3, d1))
        s = 1 if d1 in PLUS[w] else -1
        for half in (0, 1):
            w_send(w, half, d1, -s, 1, s, (4,))

    def w_last(w):
        w_got(w, 8, (4,))

    def unit(w, half, da, db):
        dz, dx = (db, da) if half == 0 else (da, db)
        return parts[w].at[rows(chunk(dz, dx), 128), half * 512 : half * 512 + 512]

    def rs_way(half, second, s):
        return way(1 - half, second, s)

    def sign(w, db):
        return 1 if db % 4 in PLUS[w] else -1

    def rs_got(w, units, stage):
        got(parts[w].at[0 : 128 * units, 0:512], ("rs", w, *stage))

    def end1(w, half, db, s):
        return (lft1 if s > 0 else rgt1).at[w, half, db]

    def end2(w, half, s):
        return (lft2 if s > 0 else rgt2).at[w, half]

    def far(w, half, db):
        send(rs_way(half, 0, sign(w, db)), unit(w, half, 2, db), fwd1.at[w, half, db], ("rs", w, 1, db))

    def rs_far(w, dz):
        far(w, 0, dz)
        if dz == 2:
            for db in (2, 1, 3, 0):
                far(w, 1, db)

    def rs_near(w, db):
        s = -sign(w, db)
        for half in (0, 1):
            send(rs_way(half, 0, s), unit(w, half, s, db), end1(w, half, db, s), ("rs", w, 2, db))

    def rs_relay(w, db):
        s = sign(w, db)
        rs_got(w, 2, (1, db))
        for half in (0, 1):
            mine = unit(w, half, s, db)
            add(mine, mine, fwd1.at[w, half, db])
            send(rs_way(half, 0, s), mine, end1(w, half, db, s), ("rs", w, 2, db))

    def rs_mid(w, db):
        s = TURN[w]
        rs_got(w, 4, (2, db))
        if db == s % 4:
            rs_got(w, 2, (3,))
        elif db == 0:
            rs_got(w, 4, (4,))
        for half in (0, 1):
            terms = [unit(w, half, 0, db), lft1.at[w, half, db], rgt1.at[w, half, db]]
            mine = sum1.at[w, half, db]
            if db == 2:
                add(mine, *terms)
                send(rs_way(half, 1, s), mine, fwd2.at[w, half], ("rs", w, 3))
            elif db == -s % 4:
                add(mine, *terms)
                send(rs_way(half, 1, -s), mine, end2(w, half, -s), ("rs", w, 4))
            elif db == s % 4:
                add(mine, *terms, fwd2.at[w, half])
                send(rs_way(half, 1, s), mine, end2(w, half, s), ("rs", w, 4))
            else:
                out = (gd_out, gu_out)[w].at[:, half * 512 : half * 512 + 512]
                add(out, *terms, lft2.at[w, half], rgt2.at[w, half], scale=factor)

    def block(df, mine):
        core = tp if mine else 1 - tp
        return (ring(fs, df) * 2 + core) * 128

    def gi_rows(df, h):
        return part_i.at[rows(block(df, True) + h * 64, 64), :]

    def gi_pair():
        for df in (2, 1, 3, 0):
            src = part_i.at[rows(block(df, False), 128), :]
            send("co", src, pair_in.at[df], ("gi", 0, df))

    def gi_got(pieces, stage):
        got(part_i.at[0 : 64 * pieces, :], ("gi", 0, stage))

    def gi_sum(df):
        gi_got(2, df)
        mine = part_i.at[rows(block(df, True), 128), :]
        add(mine, mine, pair_in.at[df], size=16)

    def gi_far():
        gi_sum(2)
        send("yp", gi_rows(2, 0), hop_f.at[0], ("gi", 0, "far"))
        send("ym", gi_rows(2, 1), hop_f.at[1], ("gi", 0, "far"))
        gi_sum(1)
        send("yp", gi_rows(1, 1), hop_l.at[1], ("gi", 0, "end"))
        gi_sum(3)
        send("ym", gi_rows(3, 0), hop_r.at[0], ("gi", 0, "end"))

    def gi_relay():
        gi_got(2, "far")
        add(gi_rows(1, 0), gi_rows(1, 0), hop_f.at[0], size=16)
        send("yp", gi_rows(1, 0), hop_l.at[0], ("gi", 0, "end"))
        add(gi_rows(3, 1), gi_rows(3, 1), hop_f.at[1], size=16)
        send("ym", gi_rows(3, 1), hop_r.at[1], ("gi", 0, "end"))

    def gi_end():
        gi_got(2, 0)
        gi_got(4, "end")
        for h in (0, 1):
            add(
                gi_out.at[pl.ds(h * 64, 64), :],
                gi_rows(0, h), pair_in.at[0, pl.ds(h * 64, 64), :], hop_l.at[h], hop_r.at[h], size=16,
            )

    def squares():
        def one(i, carry):
            r = rows(i * 32, 32)
            linear = jnp.maximum(pre[r, :].astype(F32), 0.0)
            sq[r, :] = (linear * linear).astype(BF16)
            return carry

        lax.fori_loop(0, 32, one, 0)

    def grad_tile(w, dz):
        right = (sq, gp)[w]
        start = ring(z, dz) * 512
        turned[...] = tokens[w][:, rows(start, 512)].T

        def one(j, carry):
            c = rows(j * 512, 512)
            parts[w][rows(start, 512), c] = jnp.dot(
                turned[...], right[:, c], preferred_element_type=F32
            ).astype(BF16)
            return carry

        lax.fori_loop(0, 2, one, 0)

    def pre_tile(i, half):
        def one(j, carry):
            r, c = rows(i * 512, 512), rows(half * 512 + j * 256, 256)
            acc = jnp.dot(tok_g[r, :], w_d[:, c], preferred_element_type=F32)
            linear = jnp.maximum(pre[r, c].astype(F32), 0.0)
            gp[r, c] = (acc * 2.0 * linear).astype(BF16)
            return carry

        lax.fori_loop(0, 2, one, 0)

    def term_tile(i, half):
        def one(j, carry):
            r, c = rows(i * 512, 512), rows(half * 1024 + j * 512, 512)
            part_i[r, c] = lax.dot_general(
                gp[r, :], w_u[c, :], (((1,), (1,)), ((), ())), preferred_element_type=F32
            ).astype(BF16)
            return carry

        lax.fori_loop(0, 2, one, 0)

    own = rows((fs * 2 + tp) * 128, 128)
    mine = rows(rep * 128, 128)
    local = [
        pltpu.make_async_copy(src, dst, local_sem.at[n])
        for n, (src, dst) in enumerate(
            (
                (wd_in, w_d.at[mine, :]),
                (og, tok_g.at[own, :]),
                (wu_in, w_u.at[mine, :]),
                (inp, tok_x.at[own, :]),
                (pre_in, pre),
            )
        )
    ]
    for copy in local:
        copy.start()
    barrier = pltpu.get_barrier_semaphore()
    for to in target.values():
        pl.semaphore_signal(barrier, inc=1, device_id=to, device_id_type=MESH)
    pl.semaphore_wait(barrier, len(target))

    def begin():
        local[0].wait()
        w_own(0)
        local[1].wait()
        tok_own(0)
        for n in (2, 3, 4):
            local[n].wait()

    def finish():
        for w in (0, 1):
            sent(weights[w].at[0:1920, :], ("w", w))
            sent(tokens[w].at[0:896, :], ("tok", w))
            sent(parts[w].at[0:1920, :], ("rs", w))
        sent(part_i.at[0:896, :], ("gi", 0))

    events = {f.__name__: f for f in (
        begin, squares, w_own, w_first, w_second, w_third, w_last, tok_own, tok_first, tok_second, tok_third, tok_partner,
        grad_tile, rs_far, rs_near, rs_relay, rs_mid, pre_tile, term_tile, gi_pair, gi_far, gi_relay, gi_end, finish,
    )}
    for n, (what, *args) in enumerate(PLAN):
        with jax.named_scope(":".join(str(v) for v in (what, *args)) + f"#n={n}"):
            events[what](*args)


def hand_over(gi_in, gu_in, gd_in, gi_out, gu_out, gd_out, sem):
    copies = [
        pltpu.make_async_copy(src, dst, sem.at[n])
        for n, (src, dst) in enumerate(((gi_in, gi_out), (gu_in, gu_out), (gd_in, gd_out)))
    ]
    for copy in copies:
        copy.start()
    for copy in copies:
        copy.wait()


def on_device(inputs, out_grad, pre_act, w_up, w_down_t):
    hbm = pl.BlockSpec(memory_space=pltpu.HBM)
    vmem = pl.BlockSpec(memory_space=pltpu.VMEM)
    outs = (
        jax.ShapeDtypeStruct((128, 2048), BF16),
        jax.ShapeDtypeStruct((128, 1024), F32),
        jax.ShapeDtypeStruct((128, 1024), F32),
    )

    def vm(*shape, kind=BF16):
        return pltpu.VMEM(shape, kind)

    results = pl.pallas_call(
        kernel,
        out_shape=outs,
        in_specs=[hbm] * 5,
        out_specs=(vmem,) * 3,
        scratch_shapes=[
            vm(1024, 2048), vm(1024, 2048), vm(2048, 1024), vm(2048, 1024),
            vm(1024, 1024), vm(1024, 1024), vm(1024, 1024), vm(512, 1024),
            vm(2048, 1024), vm(2048, 1024), vm(1024, 2048),
            vm(2, 2, 4, 128, 512), vm(2, 2, 4, 128, 512), vm(2, 2, 4, 128, 512), vm(2, 2, 4, 128, 512),
            vm(2, 2, 128, 512), vm(2, 2, 128, 512), vm(2, 2, 128, 512),
            vm(4, 128, 2048), vm(2, 64, 2048), vm(2, 64, 2048), vm(2, 64, 2048),
            pltpu.SemaphoreType.DMA((7,)), pltpu.SemaphoreType.DMA((50,)), pltpu.SemaphoreType.DMA((5,)),
        ],
        compiler_params=pltpu.CompilerParams(
            collective_id=0, has_side_effects=True, vmem_limit_bytes=54_000_000
        ),
        name="backward",
    )(*(pltpu.with_memory_space_constraint(v, pltpu.HBM) for v in (inputs, out_grad, pre_act, w_up, w_down_t)))
    return pl.pallas_call(
        hand_over,
        out_shape=outs,
        in_specs=[vmem] * 3,
        out_specs=(hbm,) * 3,
        scratch_shapes=[pltpu.SemaphoreType.DMA((3,))],
        compiler_params=pltpu.CompilerParams(vmem_limit_bytes=4_000_000),
        name="hand_over",
    )(*results)


def solution(mesh):
    rows_all = P(("rep", "fs", "tp"), None)
    tiles = P("rep", ("fs", "tp"))
    return jax.shard_map(
        on_device,
        mesh=mesh,
        in_specs=(rows_all, rows_all, tiles, tiles, tiles),
        out_specs=(rows_all, tiles, tiles),
        check_vma=False,
    )
```

```python
import jax
import jax.numpy as jnp
from jax import lax
from jax.experimental import pallas as pl
from jax.experimental.pallas import tpu as pltpu
from jax.sharding import PartitionSpec as P

MESH = pl.DeviceIdType.MESH
BF16, F32 = jnp.bfloat16, jnp.float32
STEP = {"zp": (1, 0), "zm": (-1, 0), "xp": (0, 1), "xm": (0, -1)}
PLUS = ((0, 2), (1, 3))
TURN = (1, -1)
PLAN = (
    ("begin",), ("w_own", 1), ("w_first", 0, 1), ("w_first", 1, 1), ("tok_first", 0), ("squares",),
    ("w_first", 1, -1), ("tok_second", 0), ("tok_own", 1), ("w_second", 0), ("tok_third", 0),
    ("w_first", 0, -1), ("tok_partner", 0), ("w_second", 1), ("grad_tile", 0, 0), ("grad_tile", 0, 2),
    ("w_third", 0, 3), ("grad_tile", 0, 1), ("w_third", 0, 0), ("w_third", 0, 2), ("grad_tile", 0, 3),
    ("w_third", 0, 1), ("rs_near", 0, 2), ("tok_second", 1), ("rs_far", 0, 2), ("w_third", 1, 1),
    ("tok_first", 1), ("w_third", 1, 3), ("rs_far", 0, 1), ("w_third", 1, 2), ("w_last", 0),
    ("pre_tile", 1, 1), ("tok_third", 1), ("pre_tile", 0, 0), ("rs_far", 0, 3), ("rs_near", 0, 1),
    ("rs_relay", 0, 2), ("pre_tile", 1, 0), ("rs_near", 0, 3), ("tok_partner", 1), ("w_third", 1, 0),
    ("pre_tile", 0, 1), ("grad_tile", 1, 1), ("rs_far", 1, 1), ("rs_relay", 0, 1), ("grad_tile", 1, 2),
    ("rs_far", 1, 2), ("grad_tile", 1, 3), ("grad_tile", 1, 0), ("rs_far", 1, 3), ("rs_near", 1, 3),
    ("w_last", 1), ("term_tile", 1, 1), ("term_tile", 1, 0), ("rs_near", 0, 0), ("rs_near", 1, 2),
    ("rs_mid", 0, 2), ("rs_far", 0, 0), ("term_tile", 0, 1), ("rs_relay", 1, 2), ("term_tile", 0, 0),
    ("gi_pair",), ("rs_far", 1, 0), ("rs_near", 1, 1), ("rs_near", 1, 0), ("rs_relay", 1, 1),
    ("rs_relay", 0, 3), ("rs_relay", 1, 3), ("gi_far",), ("rs_relay", 0, 0), ("rs_mid", 1, 2), ("gi_relay",),
    ("rs_relay", 1, 0), ("rs_mid", 0, 3), ("rs_mid", 0, 1), ("rs_mid", 1, 3), ("rs_mid", 1, 1), ("gi_end",),
    ("rs_mid", 0, 0), ("rs_mid", 1, 0), ("finish",),
)


def kernel(
    inp, og, pre_in, wu_in, wd_in, gi_out, gu_out, gd_out,
    tok_g, tok_x, w_d, w_u, pre, sq, gp, turned, part_d, part_u, part_i,
    fwd1, lft1, rgt1, sum1, fwd2, lft2, rgt2,
    pair_in, hop_f, hop_l, hop_r, send_sem, recv_sem, local_sem,
):
    rep, fs, tp = lax.axis_index("rep"), lax.axis_index("fs"), lax.axis_index("tp")
    z, x = lax.div(rep, 4), lax.rem(rep, 4)
    tokens, weights, parts = (tok_g, tok_x), (w_d, w_u), (part_d, part_u)
    factor = 1.0 / 128.0

    def ring(v, d):
        return lax.rem(v + d % 4, 4)

    target = {
        "zp": {"rep": ring(z, 1) * 4 + x},
        "zm": {"rep": ring(z, -1) * 4 + x},
        "xp": {"rep": z * 4 + ring(x, 1)},
        "xm": {"rep": z * 4 + ring(x, -1)},
        "yp": {"fs": ring(fs, 1)},
        "ym": {"fs": ring(fs, -1)},
        "co": {"tp": 1 - tp},
    }
    groups, classes = {}, {}

    def remote(to, src, dst, group, kind):
        k = classes.setdefault(kind, len(classes))
        n = groups.setdefault(group, len(groups))
        return pltpu.make_async_remote_copy(
            src_ref=src, dst_ref=dst, send_sem=send_sem.at[k], recv_sem=recv_sem.at[n],
            device_id=target[to], device_id_type=MESH,
        )

    def send(to, src, dst, group):
        remote(to, src, dst, group, (group[0], *group[1:2])).start()

    def got(like, group):
        remote("co", like, like, group, (group[0], *group[1:2])).wait_recv()

    def sent(like, kind):
        remote("co", like, like, ("w", 0, 4), kind).wait_send()

    def rows(start, size):
        return pl.ds(pl.multiple_of(start, size), size)

    def add(dst, *srcs, size=32, scale=None):
        def one(i, carry):
            r = rows(i * size, size)
            total = srcs[0][r, :].astype(F32)
            for src in srcs[1:]:
                total = total + src[r, :].astype(F32)
            if scale is not None:
                total = total * scale
            dst[r, :] = total.astype(dst.dtype)
            return carry

        lax.fori_loop(0, dst.shape[0] // size, one, 0)

    def tok(a, df, mine, h):
        core = tp if mine else 1 - tp
        return tokens[a].at[rows((ring(fs, df) * 2 + core) * 128 + h * 64, 64), :]

    def tok_y(a, df, h, s, stage):
        p = tok(a, df, True, h)
        send("yp" if s > 0 else "ym", p, p, ("tok", a, stage))

    def tok_co(a, df, h):
        p = tok(a, df, True, h)
        send("co", p, p, ("tok", a, "partner"))

    def tok_got(a, pieces, stage):
        got(tokens[a].at[0 : 64 * pieces, :], ("tok", a, stage))

    def tok_own(a):
        if a == 1:
            local[3].wait()
        tok_y(a, 0, 0, 1, 1)
        tok_y(a, 0, 1, -1, 1)
        tok_y(a, 0, 1, 1, 2)
        tok_y(a, 0, 0, -1, 2)
        tok_co(a, 0, 0)
        tok_co(a, 0, 1)

    def tok_first(a):
        tok_got(a, 2, 1)
        for df, h in ((-1, 0), (1, 1)):
            tok_y(a, df, h, -df, 3)
            tok_co(a, df, h)

    def tok_second(a):
        tok_got(a, 2, 2)
        for df, h in ((-1, 1), (1, 0)):
            tok_co(a, df, h)

    def tok_third(a):
        tok_got(a, 2, 3)
        for h in (0, 1):
            tok_co(a, 2, h)

    def tok_partner(a):
        tok_got(a, 8, "partner")

    def chunk(dz, dx):
        return (ring(z, dz) * 4 + ring(x, dx)) * 128

    def offs(half, d1, d2):
        return (d1, d2) if half == 0 else (d2, d1)

    def way(half, second, s):
        return ("zx"[half ^ second]) + ("p" if s > 0 else "m")

    def w_piece(w, half, d1, d2):
        dz, dx = offs(half, d1, d2)
        return weights[w].at[rows(chunk(dz, dx) + half * 64, 64), :]

    def w_send(w, half, d1, d2, second, s, stage):
        p = w_piece(w, half, d1, d2)
        send(way(half, second, s), p, p, ("w", w, *stage))

    def w_got(w, pieces, stage):
        got(weights[w].at[0 : 64 * pieces, :], ("w", w, *stage))

    def w_own(w):
        if w == 1:
            local[2].wait()
        for second in (0, 1):
            for half in (0, 1):
                for s in (1, -1):
                    w_send(w, half, 0, 0, second, s, (3, 0) if second else (1, s))

    def w_first(w, s):
        w_got(w, 2, (1, s))
        if s == TURN[w]:
            for half in (0, 1):
                w_send(w, half, -s, 0, 0, s, (2,))
        for half in (0, 1):
            for e in (1, -1):
                w_send(w, half, -s, 0, 1, e, (3, -s % 4))

    def w_second(w):
        w_got(w, 2, (2,))
        for half in (0, 1):
            for e in (1, -1):
                w_send(w, half, 2, 0, 1, e, (3, 2))

    def w_third(w, d1):
        w_got(w, 4, (3, d1))
        s = 1 if d1 in PLUS[w] else -1
        for half in (0, 1):
            w_send(w, half, d1, -s, 1, s, (4,))

    def w_last(w):
        w_got(w, 8, (4,))

    def unit(w, half, da, db):
        dz, dx = (db, da) if half == 0 else (da, db)
        return parts[w].at[rows(chunk(dz, dx), 128), half * 512 : half * 512 + 512]

    def rs_way(half, second, s):
        return way(1 - half, second, s)

    def sign(w, db):
        return 1 if db % 4 in PLUS[w] else -1

    def rs_got(w, units, stage):
        got(parts[w].at[0 : 128 * units, 0:512], ("rs", w, *stage))

    def end1(w, half, db, s):
        return (lft1 if s > 0 else rgt1).at[w, half, db]

    def end2(w, half, s):
        return (lft2 if s > 0 else rgt2).at[w, half]

    def far(w, half, db):
        send(rs_way(half, 0, sign(w, db)), unit(w, half, 2, db), fwd1.at[w, half, db], ("rs", w, 1, db))

    def rs_far(w, dz):
        far(w, 0, dz)
        if dz == 2:
            for db in (2, 1, 3, 0):
                far(w, 1, db)

    def rs_near(w, db):
        s = -sign(w, db)
        for half in (0, 1):
            send(rs_way(half, 0, s), unit(w, half, s, db), end1(w, half, db, s), ("rs", w, 2, db))

    def rs_relay(w, db):
        s = sign(w, db)
        rs_got(w, 2, (1, db))
        for half in (0, 1):
            mine = unit(w, half, s, db)
            add(mine, mine, fwd1.at[w, half, db])
            send(rs_way(half, 0, s), mine, end1(w, half, db, s), ("rs", w, 2, db))

    def outs(w, half):
        return (gd_out, gu_out)[w].at[:, half * 512 : half * 512 + 512]

    def rs_mid(w, db):
        s = TURN[w]
        rs_got(w, 4, (2, db))
        if db == s % 4:
            rs_got(w, 2, (3,))
        for half in (0, 1):
            terms = [unit(w, half, 0, db), lft1.at[w, half, db], rgt1.at[w, half, db]]
            mine = sum1.at[w, half, db]
            if db == 2:
                add(mine, *terms)
                send(rs_way(half, 1, s), mine, fwd2.at[w, half], ("rs", w, 3))
            elif db == -s % 4:
                add(mine, *terms)
                send(rs_way(half, 1, -s), mine, end2(w, half, -s), ("rs", w, 4))
            elif db == s % 4:
                add(mine, *terms, fwd2.at[w, half])
                send(rs_way(half, 1, s), mine, end2(w, half, s), ("rs", w, 4))
            else:
                add(outs(w, half), *terms)
        if db == 0:
            rs_got(w, 4, (4,))
            for half in (0, 1):
                add(outs(w, half), outs(w, half), lft2.at[w, half], rgt2.at[w, half], scale=factor)

    def block(df, mine):
        core = tp if mine else 1 - tp
        return (ring(fs, df) * 2 + core) * 128

    def gi_rows(df, h):
        return part_i.at[rows(block(df, True) + h * 64, 64), :]

    def gi_pair():
        for df in (2, 1, 3, 0):
            src = part_i.at[rows(block(df, False), 128), :]
            send("co", src, pair_in.at[df], ("gi", 0, df))

    def gi_got(pieces, stage):
        got(part_i.at[0 : 64 * pieces, :], ("gi", 0, stage))

    def gi_sum(df):
        gi_got(2, df)
        mine = part_i.at[rows(block(df, True), 128), :]
        add(mine, mine, pair_in.at[df], size=16)

    def gi_far():
        gi_sum(2)
        send("yp", gi_rows(2, 0), hop_f.at[0], ("gi", 0, "far"))
        send("ym", gi_rows(2, 1), hop_f.at[1], ("gi", 0, "far"))
        gi_sum(1)
        send("yp", gi_rows(1, 1), hop_l.at[1], ("gi", 0, "end"))
        gi_sum(3)
        send("ym", gi_rows(3, 0), hop_r.at[0], ("gi", 0, "end"))

    def gi_relay():
        gi_got(2, "far")
        add(gi_rows(1, 0), gi_rows(1, 0), hop_f.at[0], size=16)
        send("yp", gi_rows(1, 0), hop_l.at[0], ("gi", 0, "end"))
        add(gi_rows(3, 1), gi_rows(3, 1), hop_f.at[1], size=16)
        send("ym", gi_rows(3, 1), hop_r.at[1], ("gi", 0, "end"))

    def gi_end():
        gi_got(2, 0)
        gi_got(4, "end")
        for h in (0, 1):
            add(
                gi_out.at[pl.ds(h * 64, 64), :],
                gi_rows(0, h), pair_in.at[0, pl.ds(h * 64, 64), :], hop_l.at[h], hop_r.at[h], size=16,
            )

    def squares():
        local[4].wait()

        def one(i, carry):
            r = rows(i * 32, 32)
            linear = jnp.maximum(pre[r, :].astype(F32), 0.0)
            sq[r, :] = (linear * linear).astype(BF16)
            return carry

        lax.fori_loop(0, 32, one, 0)

    def grad_tile(w, dz):
        right = (sq, gp)[w]
        start = ring(z, dz) * 512
        turned[...] = tokens[w][:, rows(start, 512)].T

        def one(j, carry):
            c = rows(j * 512, 512)
            parts[w][rows(start, 512), c] = jnp.dot(
                turned[...], right[:, c], preferred_element_type=F32
            ).astype(BF16)
            return carry

        lax.fori_loop(0, 2, one, 0)

    def pre_tile(i, half):
        def one(j, carry):
            r, c = rows(i * 512, 512), rows(half * 512 + j * 256, 256)
            acc = jnp.dot(tok_g[r, :], w_d[:, c], preferred_element_type=F32)
            linear = jnp.maximum(pre[r, c].astype(F32), 0.0)
            gp[r, c] = (acc * 2.0 * linear).astype(BF16)
            return carry

        lax.fori_loop(0, 2, one, 0)

    def term_tile(i, half):
        def one(j, carry):
            r, c = rows(i * 512, 512), rows(half * 1024 + j * 512, 512)
            part_i[r, c] = lax.dot_general(
                gp[r, :], w_u[c, :], (((1,), (1,)), ((), ())), preferred_element_type=F32
            ).astype(BF16)
            return carry

        lax.fori_loop(0, 2, one, 0)

    own = rows((fs * 2 + tp) * 128, 128)
    mine = rows(rep * 128, 128)
    local = [
        pltpu.make_async_copy(src, dst, local_sem.at[n])
        for n, (src, dst) in enumerate(
            (
                (wd_in, w_d.at[mine, :]),
                (og, tok_g.at[own, :]),
                (wu_in, w_u.at[mine, :]),
                (inp, tok_x.at[own, :]),
                (pre_in, pre),
            )
        )
    ]
    for copy in local[:2]:
        copy.start()
    barrier = pltpu.get_barrier_semaphore()
    for to in target.values():
        pl.semaphore_signal(barrier, inc=1, device_id=to, device_id_type=MESH)
    pl.semaphore_wait(barrier, len(target))

    def begin():
        local[0].wait()
        w_own(0)
        local[1].wait()
        tok_own(0)
        for copy in local[2:]:
            copy.start()

    def finish():
        for w in (0, 1):
            sent(weights[w].at[0:1920, :], ("w", w))
            sent(tokens[w].at[0:896, :], ("tok", w))
            sent(parts[w].at[0:1920, :], ("rs", w))
        sent(part_i.at[0:896, :], ("gi", 0))

    events = {f.__name__: f for f in (
        begin, squares, w_own, w_first, w_second, w_third, w_last, tok_own, tok_first, tok_second, tok_third, tok_partner,
        grad_tile, rs_far, rs_near, rs_relay, rs_mid, pre_tile, term_tile, gi_pair, gi_far, gi_relay, gi_end, finish,
    )}
    for n, (what, *args) in enumerate(PLAN):
        with jax.named_scope(":".join(str(v) for v in (what, *args)) + f"#n={n}"):
            events[what](*args)


def hand_over(gi_in, gu_in, gd_in, gi_out, gu_out, gd_out, sem):
    copies = [
        pltpu.make_async_copy(src, dst, sem.at[n])
        for n, (src, dst) in enumerate(((gi_in, gi_out), (gu_in, gu_out), (gd_in, gd_out)))
    ]
    for copy in copies:
        copy.start()
    for copy in copies:
        copy.wait()


def on_device(inputs, out_grad, pre_act, w_up, w_down_t):
    hbm = pl.BlockSpec(memory_space=pltpu.HBM)
    vmem = pl.BlockSpec(memory_space=pltpu.VMEM)
    outs = (
        jax.ShapeDtypeStruct((128, 2048), BF16),
        jax.ShapeDtypeStruct((128, 1024), F32),
        jax.ShapeDtypeStruct((128, 1024), F32),
    )

    def vm(*shape, kind=BF16):
        return pltpu.VMEM(shape, kind)

    results = pl.pallas_call(
        kernel,
        out_shape=outs,
        in_specs=[hbm] * 5,
        out_specs=(vmem,) * 3,
        scratch_shapes=[
            vm(1024, 2048), vm(1024, 2048), vm(2048, 1024), vm(2048, 1024),
            vm(1024, 1024), vm(1024, 1024), vm(1024, 1024), vm(512, 1024),
            vm(2048, 1024), vm(2048, 1024), vm(1024, 2048),
            vm(2, 2, 4, 128, 512), vm(2, 2, 4, 128, 512), vm(2, 2, 4, 128, 512), vm(2, 2, 4, 128, 512),
            vm(2, 2, 128, 512), vm(2, 2, 128, 512), vm(2, 2, 128, 512),
            vm(4, 128, 2048), vm(2, 64, 2048), vm(2, 64, 2048), vm(2, 64, 2048),
            pltpu.SemaphoreType.DMA((7,)), pltpu.SemaphoreType.DMA((50,)), pltpu.SemaphoreType.DMA((5,)),
        ],
        compiler_params=pltpu.CompilerParams(
            collective_id=0, has_side_effects=True, vmem_limit_bytes=54_000_000
        ),
        name="backward",
    )(*(pltpu.with_memory_space_constraint(v, pltpu.HBM) for v in (inputs, out_grad, pre_act, w_up, w_down_t)))
    return pl.pallas_call(
        hand_over,
        out_shape=outs,
        in_specs=[vmem] * 3,
        out_specs=(hbm,) * 3,
        scratch_shapes=[pltpu.SemaphoreType.DMA((3,))],
        compiler_params=pltpu.CompilerParams(vmem_limit_bytes=4_000_000),
        name="hand_over",
    )(*results)


def solution(mesh):
    rows_all = P(("rep", "fs", "tp"), None)
    tiles = P("rep", ("fs", "tp"))
    return jax.shard_map(
        on_device,
        mesh=mesh,
        in_specs=(rows_all, rows_all, tiles, tiles, tiles),
        out_specs=(rows_all, tiles, tiles),
        check_vma=False,
    )
```

```python
import jax
import jax.numpy as jnp
from jax import lax
from jax.experimental import pallas as pl
from jax.experimental.pallas import tpu as pltpu
from jax.sharding import PartitionSpec as P

MESH = pl.DeviceIdType.MESH
BF16, F32 = jnp.bfloat16, jnp.float32
STEP = {"zp": (1, 0), "zm": (-1, 0), "xp": (0, 1), "xm": (0, -1)}
PLUS = ((0, 2), (1, 3))
TURN = (1, -1)
DETOUR = 16
PLAN = (
    ("begin",), ("w_own", 1), ("tok_first", 0), ("w_first", 0, -1), ("w_first", 0, 1), ("w_first", 1, -1),
    ("tok_own", 1), ("tok_second", 0), ("squares",), ("w_second", 0), ("w_third", 0, 1), ("tok_third", 0),
    ("w_first", 1, 1), ("tok_partner", 0), ("grad_tile", 0, 2), ("tok_first", 1), ("w_third", 0, 3),
    ("w_third", 0, 0), ("w_third", 0, 2), ("w_second", 1), ("grad_tile", 0, 3), ("w_third", 1, 0),
    ("rs_far", 0, 2), ("grad_tile", 0, 1), ("rs_far", 0, 3), ("grad_tile", 0, 0), ("w_last", 0),
    ("rs_near", 0, 1), ("pre_tile", 0, 1), ("w_third", 1, 1), ("w_third", 1, 2), ("rs_far", 0, 1),
    ("pre_tile", 0, 0), ("tok_third", 1), ("pre_tile", 1, 1), ("tok_second", 1), ("w_third", 1, 3),
    ("pre_tile", 1, 0), ("tok_partner", 1), ("rs_near", 0, 3), ("grad_tile", 1, 2), ("rs_relay", 0, 2),
    ("rs_far", 1, 2), ("rs_near", 0, 2), ("rs_far", 0, 0), ("grad_tile", 1, 3), ("rs_far", 1, 3),
    ("rs_relay", 0, 1), ("grad_tile", 1, 1), ("w_last", 1), ("term_tile", 1, 0), ("rs_far", 1, 1),
    ("rs_relay", 0, 3), ("term_tile", 0, 1), ("term_tile", 1, 1), ("rs_relay", 1, 2), ("rs_near", 1, 3),
    ("rs_mid", 0, 2), ("rs_near", 1, 2), ("term_tile", 0, 0), ("rs_near", 1, 1), ("gi_pair",),
    ("grad_tile", 1, 0), ("rs_relay", 1, 1), ("gi_far",), ("rs_relay", 0, 0), ("rs_mid", 0, 3),
    ("rs_far", 1, 0), ("rs_relay", 1, 3), ("rs_mid", 1, 2), ("rs_near", 0, 0), ("rs_mid", 0, 1),
    ("rs_mid", 1, 1), ("rs_near", 1, 0), ("rs_relay", 1, 0), ("gi_relay",), ("rs_mid", 1, 3),
    ("rs_mid", 0, 0), ("gi_end",), ("rs_mid", 1, 0), ("finish",),
)


def kernel(
    inp, og, pre_in, wu_in, wd_in, gi_out, gu_out, gd_out,
    tok_g, tok_x, w_d, w_u, pre, sq, gp, turned, part_d, part_u, part_i,
    fwd1, lft1, rgt1, sum1, fwd2, lft2, rgt2,
    pair_in, hop_f, hop_l, hop_r, send_sem, recv_sem, local_sem,
):
    rep, fs, tp = lax.axis_index("rep"), lax.axis_index("fs"), lax.axis_index("tp")
    z, x = lax.div(rep, 4), lax.rem(rep, 4)
    tokens, weights, parts = (tok_g, tok_x), (w_d, w_u), (part_d, part_u)
    factor = 1.0 / 128.0

    def ring(v, d):
        return lax.rem(v + d % 4, 4)

    target = {
        "zp": {"rep": ring(z, 1) * 4 + x},
        "zm": {"rep": ring(z, -1) * 4 + x},
        "xp": {"rep": z * 4 + ring(x, 1)},
        "xm": {"rep": z * 4 + ring(x, -1)},
        "yp": {"fs": ring(fs, 1)},
        "ym": {"fs": ring(fs, -1)},
        "co": {"tp": 1 - tp},
    }
    groups, classes = {}, {}

    def remote(to, src, dst, group, kind):
        k = classes.setdefault(kind, len(classes))
        n = groups.setdefault(group, len(groups))
        return pltpu.make_async_remote_copy(
            src_ref=src, dst_ref=dst, send_sem=send_sem.at[k], recv_sem=recv_sem.at[n],
            device_id=target[to] if isinstance(to, str) else to, device_id_type=MESH,
        )

    def send(to, src, dst, group):
        remote(to, src, dst, group, (group[0], *group[1:2])).start()

    def got(like, group):
        remote("co", like, like, group, (group[0], *group[1:2])).wait_recv()

    def sent(like, kind):
        remote("co", like, like, ("w", 0, 4), kind).wait_send()

    def rows(start, size):
        return pl.ds(pl.multiple_of(start, size & -size), size)

    def add(dst, *srcs, size=32, scale=None):
        def one(i, carry):
            r = rows(i * size, size)
            total = srcs[0][r, :].astype(F32)
            for src in srcs[1:]:
                total = total + src[r, :].astype(F32)
            if scale is not None:
                total = total * scale
            dst[r, :] = total.astype(dst.dtype)
            return carry

        lax.fori_loop(0, dst.shape[0] // size, one, 0)

    def tok(a, df, mine, h):
        core = tp if mine else 1 - tp
        return tokens[a].at[rows((ring(fs, df) * 2 + core) * 128 + h * 64, 64), :]

    def tok_y(a, df, h, s, stage):
        p = tok(a, df, True, h)
        send("yp" if s > 0 else "ym", p, p, ("tok", a, stage))

    def tok_co(a, df, h):
        p = tok(a, df, True, h)
        send("co", p, p, ("tok", a, "partner"))

    def tok_got(a, pieces, stage):
        got(tokens[a].at[0 : 64 * pieces, :], ("tok", a, stage))

    def tok_own(a):
        if a == 1:
            local[3].wait()
        tok_y(a, 0, 0, 1, 1)
        tok_y(a, 0, 1, -1, 1)
        tok_y(a, 0, 1, 1, 2)
        tok_y(a, 0, 0, -1, 2)
        tok_co(a, 0, 0)
        tok_co(a, 0, 1)

    def tok_first(a):
        tok_got(a, 2, 1)
        for df, h in ((-1, 0), (1, 1)):
            tok_y(a, df, h, -df, 3)
            tok_co(a, df, h)

    def tok_second(a):
        tok_got(a, 2, 2)
        for df, h in ((-1, 1), (1, 0)):
            tok_co(a, df, h)

    def tok_third(a):
        tok_got(a, 2, 3)
        for h in (0, 1):
            tok_co(a, 2, h)

    def tok_partner(a):
        tok_got(a, 8, "partner")

    def chunk(dz, dx):
        return (ring(z, dz) * 4 + ring(x, dx)) * 128

    def offs(half, d1, d2):
        return (d1, d2) if half == 0 else (d2, d1)

    def way(half, second, s):
        return ("zx"[half ^ second]) + ("p" if s > 0 else "m")

    def w_piece(w, half, d1, d2, off=0, size=64):
        dz, dx = offs(half, d1, d2)
        return weights[w].at[rows(chunk(dz, dx) + half * 64 + off, size), :]

    def w_send(w, half, d1, d2, second, s, stage):
        p = w_piece(w, half, d1, d2)
        send(way(half, second, s), p, p, ("w", w, *stage))

    def w_got(w, pieces, stage):
        got(weights[w].at[0 : 64 * pieces, :], ("w", w, *stage))

    def w_own(w):
        if w == 1:
            local[2].wait()
        for second in (0, 1):
            for half in (0, 1):
                for s in (1, -1):
                    w_send(w, half, 0, 0, second, s, (3, 0) if second else (1, s))

    def w_first(w, s):
        w_got(w, 2, (1, s))
        if s == TURN[w]:
            for half in (0, 1):
                w_send(w, half, -s, 0, 0, s, (2,))
        for half in (0, 1):
            for e in (1, -1):
                w_send(w, half, -s, 0, 1, e, (3, -s % 4))

    def w_second(w):
        w_got(w, 2, (2,))
        for half in (0, 1):
            for e in (1, -1):
                w_send(w, half, 2, 0, 1, e, (3, 2))

    def w_detour(half):
        at = (x, z)[half]
        p = w_piece(0, half, 0, -1, 0, 64 - DETOUR)
        send(way(half, 1, 1), p, p, ("w", 0, 4))
        turn = 1 - 2 * lax.rem(at, 2)
        other = lax.rem(at + turn + 4, 4)
        back = lax.rem(at - turn + 4, 4)
        start = (z * 4 + back if half == 0 else back * 4 + x) * 128 + half * 64 + 64 - DETOUR
        q = w_d.at[rows(start, DETOUR), :]
        send({"rep": z * 4 + other if half == 0 else other * 4 + x}, q, q, ("w", 0, 4))

    def w_third(w, d1):
        w_got(w, 4, (3, d1))
        s = 1 if d1 in PLUS[w] else -1
        for half in (0, 1):
            if (w, d1) == (0, 0):
                w_detour(half)
            else:
                w_send(w, half, d1, -s, 1, s, (4,))

    def w_last(w):
        w_got(w, 8, (4,))

    def unit(w, half, da, db):
        dz, dx = (db, da) if half == 0 else (da, db)
        return parts[w].at[rows(chunk(dz, dx), 128), half * 512 : half * 512 + 512]

    def rs_way(half, second, s):
        return way(1 - half, second, s)

    def sign(w, db):
        return 1 if db % 4 in PLUS[w] else -1

    def rs_got(w, units, stage):
        got(parts[w].at[0 : 128 * units, 0:512], ("rs", w, *stage))

    def end1(w, half, db, s):
        return (lft1 if s > 0 else rgt1).at[w, half, db]

    def end2(w, half, s):
        return (lft2 if s > 0 else rgt2).at[w, half]

    def far(w, half, db):
        send(rs_way(half, 0, sign(w, db)), unit(w, half, 2, db), fwd1.at[w, half, db], ("rs", w, 1, db))

    def rs_far(w, dz):
        far(w, 0, dz)
        if dz == 2:
            for db in (2, 1, 3, 0):
                far(w, 1, db)

    def rs_near(w, db):
        s = -sign(w, db)
        for half in (0, 1):
            send(rs_way(half, 0, s), unit(w, half, s, db), end1(w, half, db, s), ("rs", w, 2, db))

    def rs_relay(w, db):
        s = sign(w, db)
        rs_got(w, 2, (1, db))
        for half in (0, 1):
            mine = unit(w, half, s, db)
            add(mine, mine, fwd1.at[w, half, db])
            send(rs_way(half, 0, s), mine, end1(w, half, db, s), ("rs", w, 2, db))

    def outs(w, half):
        return (gd_out, gu_out)[w].at[:, half * 512 : half * 512 + 512]

    def rs_mid(w, db):
        s = TURN[w]
        rs_got(w, 4, (2, db))
        if db == s % 4:
            rs_got(w, 2, (3,))
        for half in (0, 1):
            terms = [unit(w, half, 0, db), lft1.at[w, half, db], rgt1.at[w, half, db]]
            mine = sum1.at[w, half, db]
            if db == 2:
                add(mine, *terms)
                send(rs_way(half, 1, s), mine, fwd2.at[w, half], ("rs", w, 3))
            elif db == -s % 4:
                add(mine, *terms)
                send(rs_way(half, 1, -s), mine, end2(w, half, -s), ("rs", w, 4))
            elif db == s % 4:
                add(mine, *terms, fwd2.at[w, half])
                send(rs_way(half, 1, s), mine, end2(w, half, s), ("rs", w, 4))
            else:
                add(outs(w, half), *terms)
        if db == 0:
            rs_got(w, 4, (4,))
            for half in (0, 1):
                add(outs(w, half), outs(w, half), lft2.at[w, half], rgt2.at[w, half], scale=factor)

    def block(df, mine):
        core = tp if mine else 1 - tp
        return (ring(fs, df) * 2 + core) * 128

    def gi_rows(df, h):
        return part_i.at[rows(block(df, True) + h * 64, 64), :]

    def gi_pair():
        for df in (2, 1, 3, 0):
            src = part_i.at[rows(block(df, False), 128), :]
            send("co", src, pair_in.at[df], ("gi", 0, df))

    def gi_got(pieces, stage):
        got(part_i.at[0 : 64 * pieces, :], ("gi", 0, stage))

    def gi_sum(df):
        gi_got(2, df)
        mine = part_i.at[rows(block(df, True), 128), :]
        add(mine, mine, pair_in.at[df], size=16)

    def gi_far():
        gi_sum(2)
        send("yp", gi_rows(2, 0), hop_f.at[0], ("gi", 0, "far"))
        send("ym", gi_rows(2, 1), hop_f.at[1], ("gi", 0, "far"))
        gi_sum(1)
        send("yp", gi_rows(1, 1), hop_l.at[1], ("gi", 0, "end"))
        gi_sum(3)
        send("ym", gi_rows(3, 0), hop_r.at[0], ("gi", 0, "end"))

    def gi_relay():
        gi_got(2, "far")
        add(gi_rows(1, 0), gi_rows(1, 0), hop_f.at[0], size=16)
        send("yp", gi_rows(1, 0), hop_l.at[0], ("gi", 0, "end"))
        add(gi_rows(3, 1), gi_rows(3, 1), hop_f.at[1], size=16)
        send("ym", gi_rows(3, 1), hop_r.at[1], ("gi", 0, "end"))

    def gi_end():
        gi_got(2, 0)
        gi_got(4, "end")
        for h in (0, 1):
            add(
                gi_out.at[pl.ds(h * 64, 64), :],
                gi_rows(0, h), pair_in.at[0, pl.ds(h * 64, 64), :], hop_l.at[h], hop_r.at[h], size=16,
            )

    def squares():
        local[4].wait()

        def one(i, carry):
            r = rows(i * 32, 32)
            linear = jnp.maximum(pre[r, :].astype(F32), 0.0)
            sq[r, :] = (linear * linear).astype(BF16)
            return carry

        lax.fori_loop(0, 32, one, 0)

    def grad_tile(w, dz):
        right = (sq, gp)[w]
        start = ring(z, dz) * 512
        turned[...] = tokens[w][:, rows(start, 512)].T

        def one(j, carry):
            c = rows(j * 512, 512)
            parts[w][rows(start, 512), c] = jnp.dot(
                turned[...], right[:, c], preferred_element_type=F32
            ).astype(BF16)
            return carry

        lax.fori_loop(0, 2, one, 0)

    def pre_tile(i, half):
        def one(j, carry):
            r, c = rows(i * 512, 512), rows(half * 512 + j * 256, 256)
            acc = jnp.dot(tok_g[r, :], w_d[:, c], preferred_element_type=F32)
            linear = jnp.maximum(pre[r, c].astype(F32), 0.0)
            gp[r, c] = (acc * 2.0 * linear).astype(BF16)
            return carry

        lax.fori_loop(0, 2, one, 0)

    def term_tile(i, half):
        def one(j, carry):
            r, c = rows(i * 512, 512), rows(half * 1024 + j * 512, 512)
            part_i[r, c] = lax.dot_general(
                gp[r, :], w_u[c, :], (((1,), (1,)), ((), ())), preferred_element_type=F32
            ).astype(BF16)
            return carry

        lax.fori_loop(0, 2, one, 0)

    own = rows((fs * 2 + tp) * 128, 128)
    mine = rows(rep * 128, 128)
    local = [
        pltpu.make_async_copy(src, dst, local_sem.at[n])
        for n, (src, dst) in enumerate(
            (
                (wd_in, w_d.at[mine, :]),
                (og, tok_g.at[own, :]),
                (wu_in, w_u.at[mine, :]),
                (inp, tok_x.at[own, :]),
                (pre_in, pre),
            )
        )
    ]
    for copy in local[:2]:
        copy.start()
    barrier = pltpu.get_barrier_semaphore()
    for to in target.values():
        pl.semaphore_signal(barrier, inc=1, device_id=to, device_id_type=MESH)
    pl.semaphore_wait(barrier, len(target))

    def begin():
        local[0].wait()
        w_own(0)
        local[1].wait()
        tok_own(0)
        for copy in local[2:]:
            copy.start()

    def finish():
        for w in (0, 1):
            sent(weights[w].at[0:1920, :], ("w", w))
            sent(tokens[w].at[0:896, :], ("tok", w))
            sent(parts[w].at[0:1920, :], ("rs", w))
        sent(part_i.at[0:896, :], ("gi", 0))

    events = {f.__name__: f for f in (
        begin, squares, w_own, w_first, w_second, w_third, w_last, tok_own, tok_first, tok_second, tok_third, tok_partner,
        grad_tile, rs_far, rs_near, rs_relay, rs_mid, pre_tile, term_tile, gi_pair, gi_far, gi_relay, gi_end, finish,
    )}
    for n, (what, *args) in enumerate(PLAN):
        with jax.named_scope(":".join(str(v) for v in (what, *args)) + f"#n={n}"):
            events[what](*args)


def hand_over(gi_in, gu_in, gd_in, gi_out, gu_out, gd_out, sem):
    copies = [
        pltpu.make_async_copy(src, dst, sem.at[n])
        for n, (src, dst) in enumerate(((gi_in, gi_out), (gu_in, gu_out), (gd_in, gd_out)))
    ]
    for copy in copies:
        copy.start()
    for copy in copies:
        copy.wait()


def on_device(inputs, out_grad, pre_act, w_up, w_down_t):
    hbm = pl.BlockSpec(memory_space=pltpu.HBM)
    vmem = pl.BlockSpec(memory_space=pltpu.VMEM)
    outs = (
        jax.ShapeDtypeStruct((128, 2048), BF16),
        jax.ShapeDtypeStruct((128, 1024), F32),
        jax.ShapeDtypeStruct((128, 1024), F32),
    )

    def vm(*shape, kind=BF16):
        return pltpu.VMEM(shape, kind)

    results = pl.pallas_call(
        kernel,
        out_shape=outs,
        in_specs=[hbm] * 5,
        out_specs=(vmem,) * 3,
        scratch_shapes=[
            vm(1024, 2048), vm(1024, 2048), vm(2048, 1024), vm(2048, 1024),
            vm(1024, 1024), vm(1024, 1024), vm(1024, 1024), vm(512, 1024),
            vm(2048, 1024), vm(2048, 1024), vm(1024, 2048),
            vm(2, 2, 4, 128, 512), vm(2, 2, 4, 128, 512), vm(2, 2, 4, 128, 512), vm(2, 2, 4, 128, 512),
            vm(2, 2, 128, 512), vm(2, 2, 128, 512), vm(2, 2, 128, 512),
            vm(4, 128, 2048), vm(2, 64, 2048), vm(2, 64, 2048), vm(2, 64, 2048),
            pltpu.SemaphoreType.DMA((7,)), pltpu.SemaphoreType.DMA((50,)), pltpu.SemaphoreType.DMA((5,)),
        ],
        compiler_params=pltpu.CompilerParams(
            collective_id=0, has_side_effects=True, vmem_limit_bytes=54_000_000
        ),
        name="backward",
    )(*(pltpu.with_memory_space_constraint(v, pltpu.HBM) for v in (inputs, out_grad, pre_act, w_up, w_down_t)))
    return pl.pallas_call(
        hand_over,
        out_shape=outs,
        in_specs=[vmem] * 3,
        out_specs=(hbm,) * 3,
        scratch_shapes=[pltpu.SemaphoreType.DMA((3,))],
        compiler_params=pltpu.CompilerParams(vmem_limit_bytes=4_000_000),
        name="hand_over",
    )(*results)


def solution(mesh):
    rows_all = P(("rep", "fs", "tp"), None)
    tiles = P("rep", ("fs", "tp"))
    return jax.shard_map(
        on_device,
        mesh=mesh,
        in_specs=(rows_all, rows_all, tiles, tiles, tiles),
        out_specs=(rows_all, tiles, tiles),
        check_vma=False,
    )
```

```python
import jax
import jax.numpy as jnp
from jax import lax
from jax.experimental import pallas as pl
from jax.experimental.pallas import tpu as pltpu
from jax.sharding import PartitionSpec as P

MESH = pl.DeviceIdType.MESH
BF16, F32 = jnp.bfloat16, jnp.float32
STEP = {"zp": (1, 0), "zm": (-1, 0), "xp": (0, 1), "xm": (0, -1)}
PLUS = ((0, 2), (1, 3))
TURN = (1, -1)
DETOUR = 16
PLAN = (
    ("begin",), ("squares",), ("w_own", 1), ("w_first", 0, -1), ("tok_first", 0), ("w_first", 0, 1),
    ("tok_own", 1), ("w_first", 1, -1), ("tok_second", 0), ("tok_third", 0), ("w_second", 0),
    ("tok_partner", 0), ("w_first", 1, 1), ("w_third", 0, 1), ("w_third", 0, 0), ("w_second", 1),
    ("grad_tile", 0, 0), ("grad_tile", 0, 3), ("grad_tile", 0, 2), ("w_third", 0, 3), ("rs_near", 0, 2),
    ("w_third", 0, 2), ("grad_tile", 0, 1), ("rs_far", 0, 2), ("w_third", 1, 0), ("tok_second", 1),
    ("tok_first", 1), ("rs_near", 0, 3), ("rs_far", 0, 3), ("rs_far", 0, 0), ("rs_far", 0, 1),
    ("w_third", 1, 2), ("w_last", 0), ("tok_third", 1), ("pre_tile", 1, 1), ("w_third", 1, 3),
    ("w_third", 1, 1), ("pre_tile", 0, 1), ("tok_partner", 1), ("pre_tile", 1, 0), ("pre_tile", 0, 0),
    ("grad_tile", 1, 2), ("rs_relay", 0, 2), ("rs_far", 1, 2), ("grad_tile", 1, 3), ("grad_tile", 1, 1),
    ("rs_near", 1, 3), ("rs_far", 1, 3), ("rs_relay", 0, 0), ("rs_relay", 0, 3), ("rs_far", 1, 1),
    ("w_last", 1), ("rs_near", 1, 2), ("term_tile", 0, 1), ("term_tile", 0, 0), ("rs_relay", 1, 2),
    ("term_tile", 1, 1), ("rs_mid", 0, 2), ("rs_relay", 0, 1), ("term_tile", 1, 0), ("gi_pair",),
    ("rs_near", 1, 1), ("rs_near", 0, 1), ("gi_far",), ("rs_relay", 1, 1), ("rs_relay", 1, 3),
    ("grad_tile", 1, 0), ("rs_far", 1, 0), ("rs_mid", 1, 2), ("rs_near", 0, 0), ("rs_mid", 0, 3),
    ("rs_near", 1, 0), ("rs_relay", 1, 0), ("gi_relay",), ("rs_mid", 0, 1), ("rs_mid", 1, 1),
    ("rs_mid", 1, 3), ("gi_end",), ("rs_mid", 0, 0), ("rs_mid", 1, 0), ("finish",),
)


def kernel(
    inp, og, pre_in, wu_in, wd_in, gi_out, gu_out, gd_out,
    tok_g, tok_x, w_d, w_u, pre, sq, gp, turned, part_d, part_u, part_i,
    fwd1, lft1, rgt1, sum1, fwd2, lft2, rgt2,
    pair_in, hop_f, hop_l, hop_r, send_sem, recv_sem, local_sem, ready_sem,
):
    rep, fs, tp = lax.axis_index("rep"), lax.axis_index("fs"), lax.axis_index("tp")
    z, x = lax.div(rep, 4), lax.rem(rep, 4)
    tokens, weights, parts = (tok_g, tok_x), (w_d, w_u), (part_d, part_u)
    factor = 1.0 / 128.0

    def ring(v, d):
        return lax.rem(v + d % 4, 4)

    target = {
        "zp": {"rep": ring(z, 1) * 4 + x},
        "zm": {"rep": ring(z, -1) * 4 + x},
        "xp": {"rep": z * 4 + ring(x, 1)},
        "xm": {"rep": z * 4 + ring(x, -1)},
        "yp": {"fs": ring(fs, 1)},
        "ym": {"fs": ring(fs, -1)},
        "co": {"tp": 1 - tp},
    }
    groups, classes = {}, {}

    def remote(to, src, dst, group, kind):
        k = classes.setdefault(kind, len(classes))
        n = groups.setdefault(group, len(groups))
        return pltpu.make_async_remote_copy(
            src_ref=src, dst_ref=dst, send_sem=send_sem.at[k], recv_sem=recv_sem.at[n],
            device_id=target[to] if isinstance(to, str) else to, device_id_type=MESH,
        )

    def send(to, src, dst, group):
        remote(to, src, dst, group, (group[0], *group[1:2])).start()

    def got(like, group):
        remote("co", like, like, group, (group[0], *group[1:2])).wait_recv()

    def sent(like, kind):
        remote("co", like, like, ("w", 0, 4), kind).wait_send()

    def rows(start, size):
        return pl.ds(pl.multiple_of(start, size & -size), size)

    def add(dst, *srcs, size=32, scale=None):
        def one(i, carry):
            r = rows(i * size, size)
            total = srcs[0][r, :].astype(F32)
            for src in srcs[1:]:
                total = total + src[r, :].astype(F32)
            if scale is not None:
                total = total * scale
            dst[r, :] = total.astype(dst.dtype)
            return carry

        lax.fori_loop(0, dst.shape[0] // size, one, 0)

    def tok(a, df, mine, h):
        core = tp if mine else 1 - tp
        return tokens[a].at[rows((ring(fs, df) * 2 + core) * 128 + h * 64, 64), :]

    def tok_y(a, df, h, s, stage):
        p = tok(a, df, True, h)
        send("yp" if s > 0 else "ym", p, p, ("tok", a, stage))

    def tok_co(a, df, h):
        p = tok(a, df, True, h)
        send("co", p, p, ("tok", a, "partner"))

    def tok_got(a, pieces, stage):
        got(tokens[a].at[0 : 64 * pieces, :], ("tok", a, stage))

    def tok_own(a):
        if a == 1:
            local[3].wait()
        tok_y(a, 0, 0, 1, 1)
        tok_y(a, 0, 1, -1, 1)
        tok_y(a, 0, 1, 1, 2)
        tok_y(a, 0, 0, -1, 2)
        tok_co(a, 0, 0)
        tok_co(a, 0, 1)

    def tok_first(a):
        tok_got(a, 2, 1)
        for df, h in ((-1, 0), (1, 1)):
            tok_y(a, df, h, -df, 3)
            tok_co(a, df, h)

    def tok_second(a):
        tok_got(a, 2, 2)
        for df, h in ((-1, 1), (1, 0)):
            tok_co(a, df, h)

    def tok_third(a):
        tok_got(a, 2, 3)
        for h in (0, 1):
            tok_co(a, 2, h)

    def tok_partner(a):
        tok_got(a, 8, "partner")

    def chunk(dz, dx):
        return (ring(z, dz) * 4 + ring(x, dx)) * 128

    def offs(half, d1, d2):
        return (d1, d2) if half == 0 else (d2, d1)

    def way(half, second, s):
        return ("zx"[half ^ second]) + ("p" if s > 0 else "m")

    def w_piece(w, half, d1, d2, off=0, size=64):
        dz, dx = offs(half, d1, d2)
        return weights[w].at[rows(chunk(dz, dx) + half * 64 + off, size), :]

    def w_send(w, half, d1, d2, second, s, stage):
        p = w_piece(w, half, d1, d2)
        send(way(half, second, s), p, p, ("w", w, *stage))

    def w_got(w, pieces, stage):
        got(weights[w].at[0 : 64 * pieces, :], ("w", w, *stage))

    def w_own(w):
        if w == 1:
            local[2].wait()
        for second in (0, 1):
            for half in (0, 1):
                for s in (1, -1):
                    w_send(w, half, 0, 0, second, s, (3, 0) if second else (1, s))

    def w_own_along(axis):
        for second in (0, 1):
            half = second if axis == "z" else 1 - second
            for s in (1, -1):
                w_send(0, half, 0, 0, second, s, (3, 0) if second else (1, s))

    def w_first(w, s):
        w_got(w, 2, (1, s))
        if s == TURN[w]:
            for half in (0, 1):
                w_send(w, half, -s, 0, 0, s, (2,))
        for half in (0, 1):
            for e in (1, -1):
                w_send(w, half, -s, 0, 1, e, (3, -s % 4))

    def w_second(w):
        w_got(w, 2, (2,))
        for half in (0, 1):
            for e in (1, -1):
                w_send(w, half, 2, 0, 1, e, (3, 2))

    def w_detour(half):
        at = (x, z)[half]
        p = w_piece(0, half, 0, -1, 0, 64 - DETOUR)
        send(way(half, 1, 1), p, p, ("w", 0, 4))
        turn = 1 - 2 * lax.rem(at, 2)
        other = lax.rem(at + turn + 4, 4)
        back = lax.rem(at - turn + 4, 4)
        start = (z * 4 + back if half == 0 else back * 4 + x) * 128 + half * 64 + 64 - DETOUR
        q = w_d.at[rows(start, DETOUR), :]
        send({"rep": z * 4 + other if half == 0 else other * 4 + x}, q, q, ("w", 0, 4))

    def w_third(w, d1):
        w_got(w, 4, (3, d1))
        s = 1 if d1 in PLUS[w] else -1
        for half in (0, 1):
            if (w, d1) == (0, 0):
                w_detour(half)
            else:
                w_send(w, half, d1, -s, 1, s, (4,))

    def w_last(w):
        w_got(w, 8, (4,))

    def unit(w, half, da, db):
        dz, dx = (db, da) if half == 0 else (da, db)
        return parts[w].at[rows(chunk(dz, dx), 128), half * 512 : half * 512 + 512]

    def rs_way(half, second, s):
        return way(1 - half, second, s)

    def sign(w, db):
        return 1 if db % 4 in PLUS[w] else -1

    def rs_got(w, units, stage):
        got(parts[w].at[0 : 128 * units, 0:512], ("rs", w, *stage))

    def end1(w, half, db, s):
        return (lft1 if s > 0 else rgt1).at[w, half, db]

    def end2(w, half, s):
        return (lft2 if s > 0 else rgt2).at[w, half]

    def far(w, half, db):
        send(rs_way(half, 0, sign(w, db)), unit(w, half, 2, db), fwd1.at[w, half, db], ("rs", w, 1, db))

    def rs_far(w, dz):
        far(w, 0, dz)
        if dz == 2:
            for db in (2, 1, 3, 0):
                far(w, 1, db)

    def rs_near(w, db):
        s = -sign(w, db)
        for half in (0, 1):
            send(rs_way(half, 0, s), unit(w, half, s, db), end1(w, half, db, s), ("rs", w, 2, db))

    def rs_relay(w, db):
        s = sign(w, db)
        rs_got(w, 2, (1, db))
        for half in (0, 1):
            mine = unit(w, half, s, db)
            add(mine, mine, fwd1.at[w, half, db])
            send(rs_way(half, 0, s), mine, end1(w, half, db, s), ("rs", w, 2, db))

    def outs(w, half):
        return (gd_out, gu_out)[w].at[:, half * 512 : half * 512 + 512]

    def rs_mid(w, db):
        s = TURN[w]
        rs_got(w, 4, (2, db))
        if db == s % 4:
            rs_got(w, 2, (3,))
        for half in (0, 1):
            terms = [unit(w, half, 0, db), lft1.at[w, half, db], rgt1.at[w, half, db]]
            mine = sum1.at[w, half, db]
            if db == 2:
                add(mine, *terms)
                send(rs_way(half, 1, s), mine, fwd2.at[w, half], ("rs", w, 3))
            elif db == -s % 4:
                add(mine, *terms)
                send(rs_way(half, 1, -s), mine, end2(w, half, -s), ("rs", w, 4))
            elif db == s % 4:
                add(mine, *terms, fwd2.at[w, half])
                send(rs_way(half, 1, s), mine, end2(w, half, s), ("rs", w, 4))
            else:
                add(outs(w, half), *terms)
        if db == 0:
            rs_got(w, 4, (4,))
            for half in (0, 1):
                add(outs(w, half), outs(w, half), lft2.at[w, half], rgt2.at[w, half], scale=factor)

    def block(df, mine):
        core = tp if mine else 1 - tp
        return (ring(fs, df) * 2 + core) * 128

    def gi_rows(df, h):
        return part_i.at[rows(block(df, True) + h * 64, 64), :]

    def gi_pair():
        for df in (2, 1, 3, 0):
            src = part_i.at[rows(block(df, False), 128), :]
            send("co", src, pair_in.at[df], ("gi", 0, df))

    def gi_got(pieces, stage):
        got(part_i.at[0 : 64 * pieces, :], ("gi", 0, stage))

    def gi_sum(df):
        gi_got(2, df)
        mine = part_i.at[rows(block(df, True), 128), :]
        add(mine, mine, pair_in.at[df], size=16)

    def gi_far():
        gi_sum(2)
        send("yp", gi_rows(2, 0), hop_f.at[0], ("gi", 0, "far"))
        send("ym", gi_rows(2, 1), hop_f.at[1], ("gi", 0, "far"))
        gi_sum(1)
        send("yp", gi_rows(1, 1), hop_l.at[1], ("gi", 0, "end"))
        gi_sum(3)
        send("ym", gi_rows(3, 0), hop_r.at[0], ("gi", 0, "end"))

    def gi_relay():
        gi_got(2, "far")
        add(gi_rows(1, 0), gi_rows(1, 0), hop_f.at[0], size=16)
        send("yp", gi_rows(1, 0), hop_l.at[0], ("gi", 0, "end"))
        add(gi_rows(3, 1), gi_rows(3, 1), hop_f.at[1], size=16)
        send("ym", gi_rows(3, 1), hop_r.at[1], ("gi", 0, "end"))

    def gi_end():
        gi_got(2, 0)
        gi_got(4, "end")
        for h in (0, 1):
            add(
                gi_out.at[pl.ds(h * 64, 64), :],
                gi_rows(0, h), pair_in.at[0, pl.ds(h * 64, 64), :], hop_l.at[h], hop_r.at[h], size=16,
            )

    def squares():
        local[4].wait()

        def one(i, carry):
            r = rows(i * 32, 32)
            linear = jnp.maximum(pre[r, :].astype(F32), 0.0)
            sq[r, :] = (linear * linear).astype(BF16)
            return carry

        lax.fori_loop(0, 32, one, 0)

    def grad_tile(w, dz):
        right = (sq, gp)[w]
        start = ring(z, dz) * 512
        turned[...] = tokens[w][:, rows(start, 512)].T

        def one(j, carry):
            c = rows(j * 512, 512)
            parts[w][rows(start, 512), c] = jnp.dot(
                turned[...], right[:, c], preferred_element_type=F32
            ).astype(BF16)
            return carry

        lax.fori_loop(0, 2, one, 0)

    def pre_tile(i, half):
        def one(j, carry):
            r, c = rows(i * 512, 512), rows(half * 512 + j * 256, 256)
            acc = jnp.dot(tok_g[r, :], w_d[:, c], preferred_element_type=F32)
            linear = jnp.maximum(pre[r, c].astype(F32), 0.0)
            gp[r, c] = (acc * 2.0 * linear).astype(BF16)
            return carry

        lax.fori_loop(0, 2, one, 0)

    def term_tile(i, half):
        def one(j, carry):
            r, c = rows(i * 512, 512), rows(half * 1024 + j * 512, 512)
            part_i[r, c] = lax.dot_general(
                gp[r, :], w_u[c, :], (((1,), (1,)), ((), ())), preferred_element_type=F32
            ).astype(BF16)
            return carry

        lax.fori_loop(0, 2, one, 0)

    own = rows((fs * 2 + tp) * 128, 128)
    mine = rows(rep * 128, 128)
    local = [
        pltpu.make_async_copy(src, dst, local_sem.at[n])
        for n, (src, dst) in enumerate(
            (
                (wd_in, w_d.at[mine, :]),
                (og, tok_g.at[own, :]),
                (wu_in, w_u.at[mine, :]),
                (inp, tok_x.at[own, :]),
                (pre_in, pre),
            )
        )
    ]
    for copy in local[:2]:
        copy.start()
    barrier = pltpu.get_barrier_semaphore()
    for name, to in target.items():
        to = to if name == "co" else {**to, "tp": 0 if name[0] == "z" else 1}
        pl.semaphore_signal(barrier, inc=1, device_id=to, device_id_type=MESH)

    def gather():
        pl.semaphore_wait(barrier, 5 + 4 * tp)
        pl.semaphore_signal(ready_sem, inc=1, device_id=target["co"], device_id_type=MESH)

    def hear():
        pl.semaphore_wait(ready_sem, 1)

    def along_z():
        w_own_along("z")

    def along_xy():
        w_own_along("x")
        tok_own(0)

    def begin():
        local[0].wait()
        local[1].wait()
        later = lax.div(z + 3, 4)
        pl.when(tp + later == 1)(gather)
        pl.when(tp + later != 1)(hear)
        pl.when(later == 1)(along_z)
        pl.when(later == 0)(along_xy)
        pl.when(tp + later == 1)(hear)
        pl.when(tp + later != 1)(gather)
        pl.when(later == 1)(along_xy)
        pl.when(later == 0)(along_z)
        for copy in local[2:]:
            copy.start()

    def finish():
        for w in (0, 1):
            sent(weights[w].at[0:1920, :], ("w", w))
            sent(tokens[w].at[0:896, :], ("tok", w))
            sent(parts[w].at[0:1920, :], ("rs", w))
        sent(part_i.at[0:896, :], ("gi", 0))

    events = {f.__name__: f for f in (
        begin, squares, w_own, w_first, w_second, w_third, w_last, tok_own, tok_first, tok_second, tok_third, tok_partner,
        grad_tile, rs_far, rs_near, rs_relay, rs_mid, pre_tile, term_tile, gi_pair, gi_far, gi_relay, gi_end, finish,
    )}
    for n, (what, *args) in enumerate(PLAN):
        with jax.named_scope(":".join(str(v) for v in (what, *args)) + f"#n={n}"):
            events[what](*args)


def hand_over(gi_in, gu_in, gd_in, gi_out, gu_out, gd_out, sem):
    copies = [
        pltpu.make_async_copy(src, dst, sem.at[n])
        for n, (src, dst) in enumerate(((gi_in, gi_out), (gu_in, gu_out), (gd_in, gd_out)))
    ]
    for copy in copies:
        copy.start()
    for copy in copies:
        copy.wait()


def on_device(inputs, out_grad, pre_act, w_up, w_down_t):
    hbm = pl.BlockSpec(memory_space=pltpu.HBM)
    vmem = pl.BlockSpec(memory_space=pltpu.VMEM)
    outs = (
        jax.ShapeDtypeStruct((128, 2048), BF16),
        jax.ShapeDtypeStruct((128, 1024), F32),
        jax.ShapeDtypeStruct((128, 1024), F32),
    )

    def vm(*shape, kind=BF16):
        return pltpu.VMEM(shape, kind)

    results = pl.pallas_call(
        kernel,
        out_shape=outs,
        in_specs=[hbm] * 5,
        out_specs=(vmem,) * 3,
        scratch_shapes=[
            vm(1024, 2048), vm(1024, 2048), vm(2048, 1024), vm(2048, 1024),
            vm(1024, 1024), vm(1024, 1024), vm(1024, 1024), vm(512, 1024),
            vm(2048, 1024), vm(2048, 1024), vm(1024, 2048),
            vm(2, 2, 4, 128, 512), vm(2, 2, 4, 128, 512), vm(2, 2, 4, 128, 512), vm(2, 2, 4, 128, 512),
            vm(2, 2, 128, 512), vm(2, 2, 128, 512), vm(2, 2, 128, 512),
            vm(4, 128, 2048), vm(2, 64, 2048), vm(2, 64, 2048), vm(2, 64, 2048),
            pltpu.SemaphoreType.DMA((7,)), pltpu.SemaphoreType.DMA((50,)), pltpu.SemaphoreType.DMA((5,)),
            pltpu.SemaphoreType.REGULAR,
        ],
        compiler_params=pltpu.CompilerParams(
            collective_id=0, has_side_effects=True, vmem_limit_bytes=54_000_000
        ),
        name="backward",
    )(*(pltpu.with_memory_space_constraint(v, pltpu.HBM) for v in (inputs, out_grad, pre_act, w_up, w_down_t)))
    return pl.pallas_call(
        hand_over,
        out_shape=outs,
        in_specs=[vmem] * 3,
        out_specs=(hbm,) * 3,
        scratch_shapes=[pltpu.SemaphoreType.DMA((3,))],
        compiler_params=pltpu.CompilerParams(vmem_limit_bytes=4_000_000),
        name="hand_over",
    )(*results)


def solution(mesh):
    rows_all = P(("rep", "fs", "tp"), None)
    tiles = P("rep", ("fs", "tp"))
    return jax.shard_map(
        on_device,
        mesh=mesh,
        in_specs=(rows_all, rows_all, tiles, tiles, tiles),
        out_specs=(rows_all, tiles, tiles),
        check_vma=False,
    )
```

```python
import jax
import jax.numpy as jnp
from jax import lax
from jax.experimental import pallas as pl
from jax.experimental.pallas import tpu as pltpu
from jax.sharding import PartitionSpec as P

MESH = pl.DeviceIdType.MESH
BF16, F32 = jnp.bfloat16, jnp.float32
STEP = {"zp": (1, 0), "zm": (-1, 0), "xp": (0, 1), "xm": (0, -1)}
PLUS = ((0, 2), (1, 3))
TURN = (1, -1)
DETOUR = 16
PLAN = (
    ("begin",), ("squares",), ("w_own", 1), ("w_first", 0, -1), ("tok_first", 0), ("w_first", 0, 1),
    ("tok_own", 1), ("w_first", 1, -1), ("tok_second", 0), ("tok_third", 0), ("w_second", 0),
    ("tok_partner", 0), ("w_first", 1, 1), ("w_third", 0, 1), ("w_third", 0, 0), ("w_second", 1),
    ("grad_tile", 0, 0), ("grad_tile", 0, 3), ("grad_tile", 0, 2), ("w_third", 0, 3), ("rs_near", 0, 2),
    ("w_third", 0, 2), ("grad_tile", 0, 1), ("rs_far", 0, 2), ("w_third", 1, 0), ("tok_second", 1),
    ("tok_first", 1), ("rs_near", 0, 3), ("rs_far", 0, 3), ("rs_far", 0, 0), ("rs_far", 0, 1),
    ("w_third", 1, 2), ("w_last", 0), ("tok_third", 1), ("pre_tile", 1, 1), ("w_third", 1, 3),
    ("w_third", 1, 1), ("pre_tile", 0, 1), ("tok_partner", 1), ("pre_tile", 1, 0), ("pre_tile", 0, 0),
    ("grad_tile", 1, 2), ("rs_relay", 0, 2), ("rs_far", 1, 2), ("grad_tile", 1, 3), ("grad_tile", 1, 1),
    ("rs_near", 1, 3), ("rs_far", 1, 3), ("rs_relay", 0, 0), ("rs_relay", 0, 3), ("rs_far", 1, 1),
    ("w_last", 1), ("rs_near", 1, 2), ("term_tile", 0, 1), ("term_tile", 0, 0), ("rs_relay", 1, 2),
    ("term_tile", 1, 1), ("rs_mid", 0, 2), ("rs_relay", 0, 1), ("term_tile", 1, 0), ("gi_pair",),
    ("rs_near", 1, 1), ("rs_near", 0, 1), ("gi_far",), ("rs_relay", 1, 1), ("rs_relay", 1, 3),
    ("grad_tile", 1, 0), ("rs_far", 1, 0), ("rs_mid", 1, 2), ("rs_near", 0, 0), ("rs_mid", 0, 3),
    ("rs_near", 1, 0), ("rs_relay", 1, 0), ("gi_relay",), ("rs_mid", 0, 1), ("rs_mid", 1, 1),
    ("rs_mid", 1, 3), ("gi_end",), ("rs_mid", 0, 0), ("rs_mid", 1, 0), ("finish",),
)


def kernel(
    inp, og, pre_in, wu_in, wd_in, gi_out, gu_out, gd_out,
    toks, mats, pre, sq, gp, turned, sums, part_i,
    fwd1, lft1, rgt1, sum1, fwd2, lft2, rgt2,
    pair_in, hop_f, hop_l, hop_r, send_sem, recv_sem, local_sem, ready_sem,
):
    rep, fs, tp = lax.axis_index("rep"), lax.axis_index("fs"), lax.axis_index("tp")
    z, x = lax.div(rep, 4), lax.rem(rep, 4)
    tokens, weights, parts = [[ref.at[0], ref.at[1]] for ref in (toks, mats, sums)]
    (tok_g, tok_x), (w_d, w_u) = tokens, weights
    factor = 1.0 / 128.0

    def ring(v, d):
        return lax.rem(v + d % 4, 4)

    target = {
        "zp": {"rep": ring(z, 1) * 4 + x},
        "zm": {"rep": ring(z, -1) * 4 + x},
        "xp": {"rep": z * 4 + ring(x, 1)},
        "xm": {"rep": z * 4 + ring(x, -1)},
        "yp": {"fs": ring(fs, 1)},
        "ym": {"fs": ring(fs, -1)},
        "co": {"tp": 1 - tp},
    }
    groups, classes = {}, {}

    def remote(to, src, dst, group, kind):
        k = classes.setdefault(kind, len(classes))
        n = groups.setdefault(group, len(groups))
        return pltpu.make_async_remote_copy(
            src_ref=src, dst_ref=dst, send_sem=send_sem.at[k], recv_sem=recv_sem.at[n],
            device_id=target[to] if isinstance(to, str) else to, device_id_type=MESH,
        )

    def send(to, src, dst, group):
        remote(to, src, dst, group, group[0]).start()

    def got(like, group):
        remote("co", like, like, group, group[0]).wait_recv()

    def here(count, n):
        like = w_u.at[0:count, :]
        pltpu.make_async_copy(like, like, local_sem.at[n]).wait()

    def sent(like, kind):
        remote("co", like, like, ("w", 0, 4), kind).wait_send()

    def rows(start, size):
        return pl.ds(pl.multiple_of(start, size & -size), size)

    def add(dst, *srcs, size=32, scale=None):
        def one(i, carry):
            r = rows(i * size, size)
            total = srcs[0][r, :].astype(F32)
            for src in srcs[1:]:
                total = total + src[r, :].astype(F32)
            if scale is not None:
                total = total * scale
            dst[r, :] = total.astype(dst.dtype)
            return carry

        lax.fori_loop(0, dst.shape[0] // size, one, 0)

    def tok(a, df, mine, h):
        core = tp if mine else 1 - tp
        return tokens[a].at[rows((ring(fs, df) * 2 + core) * 128 + h * 64, 64), :]

    def tok_y(a, df, h, s, stage):
        p = tok(a, df, True, h)
        send("yp" if s > 0 else "ym", p, p, ("tok", a, stage))

    def tok_co(a, df, h):
        p = tok(a, df, True, h)
        send("co", p, p, ("tok", a, "partner"))

    def tok_got(a, pieces, stage):
        got(tokens[a].at[0 : 64 * pieces, :], ("tok", a, stage))

    def tok_own(a):
        tok_y(a, 0, 0, 1, 1)
        tok_y(a, 0, 1, -1, 1)
        tok_y(a, 0, 1, 1, 2)
        tok_y(a, 0, 0, -1, 2)
        tok_co(a, 0, 0)
        tok_co(a, 0, 1)

    def tok_first(a):
        tok_got(a, 2, 1)
        for df, h in ((-1, 0), (1, 1)):
            tok_y(a, df, h, -df, 3)
            tok_co(a, df, h)

    def tok_second(a):
        tok_got(a, 2, 2)
        for df, h in ((-1, 1), (1, 0)):
            tok_co(a, df, h)

    def tok_third(a):
        tok_got(a, 2, 3)
        for h in (0, 1):
            tok_co(a, 2, h)

    def tok_partner(a):
        tok_got(a, 8, "partner")

    def chunk(dz, dx):
        return (ring(z, dz) * 4 + ring(x, dx)) * 128

    def offs(half, d1, d2):
        return (d1, d2) if half == 0 else (d2, d1)

    def way(half, second, s):
        return ("zx"[half ^ second]) + ("p" if s > 0 else "m")

    def w_piece(w, half, d1, d2, off=0, size=64):
        dz, dx = offs(half, d1, d2)
        return weights[w].at[rows(chunk(dz, dx) + half * 64 + off, size), :]

    def w_send(w, half, d1, d2, second, s, stage):
        p = w_piece(w, half, d1, d2)
        send(way(half, second, s), p, p, ("w", w, *stage))

    def w_got(w, pieces, stage):
        got(weights[w].at[0 : 64 * pieces, :], ("w", w, *stage))

    def w_own(w):
        for second in (0, 1):
            for half in (0, 1):
                for s in (1, -1):
                    w_send(w, half, 0, 0, second, s, (3, 0) if second else (1, s))

    def w_own_along(axis):
        for second in (0, 1):
            half = second if axis == "z" else 1 - second
            for s in (1, -1):
                w_send(0, half, 0, 0, second, s, (3, 0) if second else (1, s))

    def w_first(w, s):
        w_got(w, 2, (1, s))
        if s == TURN[w]:
            for half in (0, 1):
                w_send(w, half, -s, 0, 0, s, (2,))
        for half in (0, 1):
            for e in (1, -1):
                w_send(w, half, -s, 0, 1, e, (3, -s % 4))

    def w_second(w):
        w_got(w, 2, (2,))
        for half in (0, 1):
            for e in (1, -1):
                w_send(w, half, 2, 0, 1, e, (3, 2))

    def w_detour(half):
        at = (x, z)[half]
        p = w_piece(0, half, 0, -1, 0, 64 - DETOUR)
        send(way(half, 1, 1), p, p, ("w", 0, 4))
        turn = 1 - 2 * lax.rem(at, 2)
        other = lax.rem(at + turn + 4, 4)
        back = lax.rem(at - turn + 4, 4)
        start = (z * 4 + back if half == 0 else back * 4 + x) * 128 + half * 64 + 64 - DETOUR
        q = w_d.at[rows(start, DETOUR), :]
        send({"rep": z * 4 + other if half == 0 else other * 4 + x}, q, q, ("w", 0, 4))

    def w_third(w, d1):
        w_got(w, 4, (3, d1))
        s = 1 if d1 in PLUS[w] else -1
        for half in (0, 1):
            if (w, d1) == (0, 0):
                w_detour(half)
            else:
                w_send(w, half, d1, -s, 1, s, (4,))

    def w_last(w):
        w_got(w, 8, (4,))

    def unit(w, half, da, db):
        dz, dx = (db, da) if half == 0 else (da, db)
        return parts[w].at[rows(chunk(dz, dx), 128), half * 512 : half * 512 + 512]

    def rs_way(half, second, s):
        return way(1 - half, second, s)

    def sign(w, db):
        return 1 if db % 4 in PLUS[w] else -1

    def rs_got(w, units, stage):
        got(parts[w].at[0 : 128 * units, 0:512], ("rs", w, *stage))

    def end1(w, half, db, s):
        return (lft1 if s > 0 else rgt1).at[w, half, db]

    def end2(w, half, s):
        return (lft2 if s > 0 else rgt2).at[w, half]

    def far(w, half, db):
        send(rs_way(half, 0, sign(w, db)), unit(w, half, 2, db), fwd1.at[w, half, db], ("rs", w, 1, db))

    def rs_far(w, dz):
        far(w, 0, dz)
        if dz == 2:
            for db in (2, 1, 3, 0):
                far(w, 1, db)

    def rs_near(w, db):
        s = -sign(w, db)
        for half in (0, 1):
            send(rs_way(half, 0, s), unit(w, half, s, db), end1(w, half, db, s), ("rs", w, 2, db))

    def rs_relay(w, db):
        s = sign(w, db)
        rs_got(w, 2, (1, db))
        for half in (0, 1):
            mine = unit(w, half, s, db)
            add(mine, mine, fwd1.at[w, half, db])
            send(rs_way(half, 0, s), mine, end1(w, half, db, s), ("rs", w, 2, db))

    def outs(w, half):
        return (gd_out, gu_out)[w].at[:, half * 512 : half * 512 + 512]

    def rs_mid(w, db):
        s = TURN[w]
        rs_got(w, 6 if db == s % 4 else 4, (2, db))
        for half in (0, 1):
            terms = [unit(w, half, 0, db), lft1.at[w, half, db], rgt1.at[w, half, db]]
            mine = sum1.at[w, half, db]
            if db == 2:
                add(mine, *terms)
                send(rs_way(half, 1, s), mine, fwd2.at[w, half], ("rs", w, 2, s % 4))
            elif db == -s % 4:
                add(mine, *terms)
                send(rs_way(half, 1, -s), mine, end2(w, half, -s), ("rs", w, 4))
            elif db == s % 4:
                add(mine, *terms, fwd2.at[w, half])
                send(rs_way(half, 1, s), mine, end2(w, half, s), ("rs", w, 4))
            else:
                add(outs(w, half), *terms)
        if db == 0:
            rs_got(w, 4, (4,))
            for half in (0, 1):
                add(outs(w, half), outs(w, half), lft2.at[w, half], rgt2.at[w, half], scale=factor)

    def block(df, mine):
        core = tp if mine else 1 - tp
        return (ring(fs, df) * 2 + core) * 128

    def gi_rows(df, h):
        return part_i.at[rows(block(df, True) + h * 64, 64), :]

    def gi_pair():
        for df in (2, 1, 3, 0):
            src = part_i.at[rows(block(df, False), 128), :]
            send("co", src, pair_in.at[df], ("gi", 0, "pair"))

    def gi_got(pieces, stage):
        got(part_i.at[0 : 64 * pieces, :], ("gi", 0, stage))

    def gi_sum(df):
        mine = part_i.at[rows(block(df, True), 128), :]
        add(mine, mine, pair_in.at[df], size=16)

    def gi_far():
        gi_got(8, "pair")
        gi_sum(2)
        send("yp", gi_rows(2, 0), hop_f.at[0], ("gi", 0, "far"))
        send("ym", gi_rows(2, 1), hop_f.at[1], ("gi", 0, "far"))
        gi_sum(1)
        send("yp", gi_rows(1, 1), hop_l.at[1], ("gi", 0, "end"))
        gi_sum(3)
        send("ym", gi_rows(3, 0), hop_r.at[0], ("gi", 0, "end"))

    def gi_relay():
        gi_got(2, "far")
        add(gi_rows(1, 0), gi_rows(1, 0), hop_f.at[0], size=16)
        send("yp", gi_rows(1, 0), hop_l.at[0], ("gi", 0, "end"))
        add(gi_rows(3, 1), gi_rows(3, 1), hop_f.at[1], size=16)
        send("ym", gi_rows(3, 1), hop_r.at[1], ("gi", 0, "end"))

    def gi_end():
        gi_got(4, "end")
        for h in (0, 1):
            add(
                gi_out.at[pl.ds(h * 64, 64), :],
                gi_rows(0, h), pair_in.at[0, pl.ds(h * 64, 64), :], hop_l.at[h], hop_r.at[h], size=16,
            )

    def squares():
        here(1408, 1)

        def one(i, carry):
            r = rows(i * 32, 32)
            linear = jnp.maximum(pre[r, :].astype(F32), 0.0)
            sq[r, :] = (linear * linear).astype(BF16)
            return carry

        lax.fori_loop(0, 32, one, 0)

    def grad_tile(w, dz):
        right = (sq, gp)[w]
        start = ring(z, dz) * 512
        turned[...] = tokens[w][:, rows(start, 512)].T

        def one(j, carry):
            c = rows(j * 512, 512)
            parts[w][rows(start, 512), c] = jnp.dot(
                turned[...], right[:, c], preferred_element_type=F32
            ).astype(BF16)
            return carry

        lax.fori_loop(0, 2, one, 0)

    def pre_tile(i, half):
        def one(j, carry):
            r, c = rows(i * 512, 512), rows(half * 512 + j * 256, 256)
            acc = jnp.dot(tok_g[r, :], w_d[:, c], preferred_element_type=F32)
            linear = jnp.maximum(pre[r, c].astype(F32), 0.0)
            gp[r, c] = (acc * 2.0 * linear).astype(BF16)
            return carry

        lax.fori_loop(0, 2, one, 0)

    def term_tile(i, half):
        def one(j, carry):
            r, c = rows(i * 512, 512), rows(half * 1024 + j * 512, 512)
            part_i[r, c] = lax.dot_general(
                gp[r, :], w_u[c, :], (((1,), (1,)), ((), ())), preferred_element_type=F32
            ).astype(BF16)
            return carry

        lax.fori_loop(0, 2, one, 0)

    own = rows((fs * 2 + tp) * 128, 128)
    mine = rows(rep * 128, 128)
    local = [
        pltpu.make_async_copy(src, dst, local_sem.at[n // 2 if n < 4 else 1])
        for n, (src, dst) in enumerate(
            (
                (wd_in, w_d.at[mine, :]),
                (og, tok_g.at[own, :]),
                (wu_in, w_u.at[mine, :]),
                (inp, tok_x.at[own, :]),
                (pre_in, pre),
            )
        )
    ]
    for copy in local[:2]:
        copy.start()
    barrier = pltpu.get_barrier_semaphore()
    for name, to in target.items():
        to = to if name == "co" else {**to, "tp": 0 if name[0] == "z" else 1}
        pl.semaphore_signal(barrier, inc=1, device_id=to, device_id_type=MESH)

    def gather():
        pl.semaphore_wait(barrier, 5 + 4 * tp)
        pl.semaphore_signal(ready_sem, inc=1, device_id=target["co"], device_id_type=MESH)

    def hear():
        pl.semaphore_wait(ready_sem, 1)

    def along_z():
        w_own_along("z")

    def along_xy():
        w_own_along("x")
        tok_own(0)

    def begin():
        here(384, 0)
        later = lax.div(z + 3, 4)
        pl.when(tp + later == 1)(gather)
        pl.when(tp + later != 1)(hear)
        pl.when(later == 1)(along_z)
        pl.when(later == 0)(along_xy)
        pl.when(tp + later == 1)(hear)
        pl.when(tp + later != 1)(gather)
        pl.when(later == 1)(along_xy)
        pl.when(later == 0)(along_z)
        for copy in local[2:]:
            copy.start()

    def finish():
        sent(mats.at[:, 0:1920, :], "w")
        sent(toks.at[:, 0:896, :], "tok")
        sent(sums.at[:, 0:1920, :], "rs")
        sent(part_i.at[0:896, :], "gi")

    events = {f.__name__: f for f in (
        begin, squares, w_own, w_first, w_second, w_third, w_last, tok_own, tok_first, tok_second, tok_third, tok_partner,
        grad_tile, rs_far, rs_near, rs_relay, rs_mid, pre_tile, term_tile, gi_pair, gi_far, gi_relay, gi_end, finish,
    )}
    for n, (what, *args) in enumerate(PLAN):
        with jax.named_scope(":".join(str(v) for v in (what, *args)) + f"#n={n}"):
            events[what](*args)


def hand_over(gi_in, gu_in, gd_in, gi_out, gu_out, gd_out, sem):
    copies = [
        pltpu.make_async_copy(src, dst, sem.at[n])
        for n, (src, dst) in enumerate(((gi_in, gi_out), (gu_in, gu_out), (gd_in, gd_out)))
    ]
    for copy in copies:
        copy.start()
    for copy in copies:
        copy.wait()


def on_device(inputs, out_grad, pre_act, w_up, w_down_t):
    hbm = pl.BlockSpec(memory_space=pltpu.HBM)
    vmem = pl.BlockSpec(memory_space=pltpu.VMEM)
    outs = (
        jax.ShapeDtypeStruct((128, 2048), BF16),
        jax.ShapeDtypeStruct((128, 1024), F32),
        jax.ShapeDtypeStruct((128, 1024), F32),
    )

    def vm(*shape, kind=BF16):
        return pltpu.VMEM(shape, kind)

    results = pl.pallas_call(
        kernel,
        out_shape=outs,
        in_specs=[hbm] * 5,
        out_specs=(vmem,) * 3,
        scratch_shapes=[
            vm(2, 1024, 2048), vm(2, 2048, 1024),
            vm(1024, 1024), vm(1024, 1024), vm(1024, 1024), vm(512, 1024),
            vm(2, 2048, 1024), vm(1024, 2048),
            vm(2, 2, 4, 128, 512), vm(2, 2, 4, 128, 512), vm(2, 2, 4, 128, 512), vm(2, 2, 4, 128, 512),
            vm(2, 2, 128, 512), vm(2, 2, 128, 512), vm(2, 2, 128, 512),
            vm(4, 128, 2048), vm(2, 64, 2048), vm(2, 64, 2048), vm(2, 64, 2048),
            pltpu.SemaphoreType.DMA((4,)), pltpu.SemaphoreType.DMA((45,)), pltpu.SemaphoreType.DMA((2,)),
            pltpu.SemaphoreType.REGULAR,
        ],
        compiler_params=pltpu.CompilerParams(
            collective_id=0, has_side_effects=True, vmem_limit_bytes=54_000_000
        ),
        name="backward",
    )(*(pltpu.with_memory_space_constraint(v, pltpu.HBM) for v in (inputs, out_grad, pre_act, w_up, w_down_t)))
    return pl.pallas_call(
        hand_over,
        out_shape=outs,
        in_specs=[vmem] * 3,
        out_specs=(hbm,) * 3,
        scratch_shapes=[pltpu.SemaphoreType.DMA((3,))],
        compiler_params=pltpu.CompilerParams(vmem_limit_bytes=4_000_000),
        name="hand_over",
    )(*results)


def solution(mesh):
    rows_all = P(("rep", "fs", "tp"), None)
    tiles = P("rep", ("fs", "tp"))
    return jax.shard_map(
        on_device,
        mesh=mesh,
        in_specs=(rows_all, rows_all, tiles, tiles, tiles),
        out_specs=(rows_all, tiles, tiles),
        check_vma=False,
    )
```

```python
import jax
import jax.numpy as jnp
from jax import lax
from jax.experimental import pallas as pl
from jax.experimental.pallas import tpu as pltpu
from jax.sharding import PartitionSpec as P

MESH = pl.DeviceIdType.MESH
BF16, F32 = jnp.bfloat16, jnp.float32
STEP = {"zp": (1, 0), "zm": (-1, 0), "xp": (0, 1), "xm": (0, -1)}
PLUS = ((0, 2), (1, 3))
TURN = (1, -1)
DETOUR = 16
FACTOR = 1.0 / 128.0
PLAN = (
    ("begin",), ("squares",), ("w_own", 1), ("w_first", 0, -1), ("tok_first", 0), ("w_first", 0, 1),
    ("tok_own", 1), ("w_first", 1, -1), ("tok_second", 0), ("tok_third", 0), ("w_second", 0),
    ("tok_partner", 0), ("w_first", 1, 1), ("w_third", 0, 1), ("w_third", 0, 0), ("w_second", 1),
    ("grad_tile", 0, 0), ("grad_tile", 0, 3), ("grad_tile", 0, 2), ("w_third", 0, 3), ("rs_near", 0, 2),
    ("w_third", 0, 2), ("grad_tile", 0, 1), ("rs_far", 0, 2), ("w_third", 1, 0), ("tok_second", 1),
    ("tok_first", 1), ("rs_near", 0, 3), ("rs_far", 0, 3), ("rs_far", 0, 0), ("rs_far", 0, 1),
    ("w_third", 1, 2), ("w_last", 0), ("tok_third", 1), ("pre_tile", 1, 1), ("w_third", 1, 3),
    ("w_third", 1, 1), ("pre_tile", 0, 1), ("tok_partner", 1), ("pre_tile", 1, 0), ("pre_tile", 0, 0),
    ("grad_tile", 1, 2), ("rs_relay", 0, 2), ("rs_far", 1, 2), ("grad_tile", 1, 3), ("grad_tile", 1, 1),
    ("rs_near", 1, 3), ("rs_far", 1, 3), ("rs_relay", 0, 0), ("rs_relay", 0, 3), ("rs_far", 1, 1),
    ("w_last", 1), ("rs_near", 1, 2), ("term_tile", 0, 1), ("term_tile", 0, 0), ("rs_relay", 1, 2),
    ("term_tile", 1, 1), ("rs_mid", 0, 2), ("rs_relay", 0, 1), ("term_tile", 1, 0), ("gi_pair",),
    ("rs_near", 1, 1), ("rs_near", 0, 1), ("gi_far",), ("rs_relay", 1, 1), ("rs_relay", 1, 3),
    ("grad_tile", 1, 0), ("rs_far", 1, 0), ("rs_mid", 1, 2), ("rs_near", 0, 0), ("rs_mid", 0, 3),
    ("rs_near", 1, 0), ("rs_relay", 1, 0), ("gi_relay",), ("rs_mid", 0, 1), ("rs_mid", 1, 1),
    ("rs_mid", 1, 3), ("gi_end",), ("rs_mid", 0, 0), ("rs_mid", 1, 0), ("finish",),
)


def kernel(
    inp, og, pre_in, wu_in, wd_in, gi_out, gu_out, gd_out, lft_out, rgt_out,
    toks, mats, pre, sq, gp, turned, sums, part_i,
    fwd1, lft1, rgt1, sum1, fwd2, lft2, rgt2,
    pair_in, hop_f, hop_l, hop_r, send_sem, recv_sem, local_sem, ready_sem,
):
    rep, fs, tp = lax.axis_index("rep"), lax.axis_index("fs"), lax.axis_index("tp")
    z, x = lax.div(rep, 4), lax.rem(rep, 4)
    tokens, weights, parts = [[ref.at[0], ref.at[1]] for ref in (toks, mats, sums)]
    (tok_g, tok_x), (w_d, w_u) = tokens, weights
    factor = FACTOR

    def ring(v, d):
        return lax.rem(v + d % 4, 4)

    target = {
        "zp": {"rep": ring(z, 1) * 4 + x},
        "zm": {"rep": ring(z, -1) * 4 + x},
        "xp": {"rep": z * 4 + ring(x, 1)},
        "xm": {"rep": z * 4 + ring(x, -1)},
        "yp": {"fs": ring(fs, 1)},
        "ym": {"fs": ring(fs, -1)},
        "co": {"tp": 1 - tp},
    }
    groups, classes = {}, {}

    def remote(to, src, dst, group, kind):
        k = classes.setdefault(kind, len(classes))
        n = groups.setdefault(group, len(groups))
        return pltpu.make_async_remote_copy(
            src_ref=src, dst_ref=dst, send_sem=send_sem.at[k], recv_sem=recv_sem.at[n],
            device_id=target[to] if isinstance(to, str) else to, device_id_type=MESH,
        )

    def send(to, src, dst, group):
        remote(to, src, dst, group, group[0]).start()

    def got(like, group):
        remote("co", like, like, group, group[0]).wait_recv()

    def here(count, n):
        like = w_u.at[0:count, :]
        pltpu.make_async_copy(like, like, local_sem.at[n]).wait()

    def sent(like, kind):
        remote("co", like, like, ("w", 0, 4), kind).wait_send()

    def rows(start, size):
        return pl.ds(pl.multiple_of(start, size & -size), size)

    def add(dst, *srcs, size=32, scale=None):
        def one(i, carry):
            r = rows(i * size, size)
            total = srcs[0][r, :].astype(F32)
            for src in srcs[1:]:
                total = total + src[r, :].astype(F32)
            if scale is not None:
                total = total * scale
            dst[r, :] = total.astype(dst.dtype)
            return carry

        lax.fori_loop(0, dst.shape[0] // size, one, 0)

    def tok(a, df, mine, h):
        core = tp if mine else 1 - tp
        return tokens[a].at[rows((ring(fs, df) * 2 + core) * 128 + h * 64, 64), :]

    def tok_y(a, df, h, s, stage):
        p = tok(a, df, True, h)
        send("yp" if s > 0 else "ym", p, p, ("tok", a, stage))

    def tok_co(a, df, h):
        p = tok(a, df, True, h)
        send("co", p, p, ("tok", a, "partner"))

    def tok_got(a, pieces, stage):
        got(tokens[a].at[0 : 64 * pieces, :], ("tok", a, stage))

    def tok_own(a):
        tok_y(a, 0, 0, 1, 1)
        tok_y(a, 0, 1, -1, 1)
        tok_y(a, 0, 1, 1, 2)
        tok_y(a, 0, 0, -1, 2)
        tok_co(a, 0, 0)
        tok_co(a, 0, 1)

    def tok_first(a):
        tok_got(a, 2, 1)
        for df, h in ((-1, 0), (1, 1)):
            tok_y(a, df, h, -df, 3)
            tok_co(a, df, h)

    def tok_second(a):
        tok_got(a, 2, 2)
        for df, h in ((-1, 1), (1, 0)):
            tok_co(a, df, h)

    def tok_third(a):
        tok_got(a, 2, 3)
        for h in (0, 1):
            tok_co(a, 2, h)

    def tok_partner(a):
        tok_got(a, 8, "partner")

    def chunk(dz, dx):
        return (ring(z, dz) * 4 + ring(x, dx)) * 128

    def offs(half, d1, d2):
        return (d1, d2) if half == 0 else (d2, d1)

    def way(half, second, s):
        return ("zx"[half ^ second]) + ("p" if s > 0 else "m")

    def w_piece(w, half, d1, d2, off=0, size=64):
        dz, dx = offs(half, d1, d2)
        return weights[w].at[rows(chunk(dz, dx) + half * 64 + off, size), :]

    def w_send(w, half, d1, d2, second, s, stage):
        p = w_piece(w, half, d1, d2)
        send(way(half, second, s), p, p, ("w", w, *stage))

    def w_got(w, pieces, stage):
        got(weights[w].at[0 : 64 * pieces, :], ("w", w, *stage))

    def w_own(w):
        for second in (0, 1):
            for half in (0, 1):
                for s in (1, -1):
                    w_send(w, half, 0, 0, second, s, (3, 0) if second else (1, s))

    def w_own_along(axis):
        for second in (0, 1):
            half = second if axis == "z" else 1 - second
            for s in (1, -1):
                w_send(0, half, 0, 0, second, s, (3, 0) if second else (1, s))

    def w_first(w, s):
        w_got(w, 2, (1, s))
        if s == TURN[w]:
            for half in (0, 1):
                w_send(w, half, -s, 0, 0, s, (2,))
        for half in (0, 1):
            for e in (1, -1):
                w_send(w, half, -s, 0, 1, e, (3, -s % 4))

    def w_second(w):
        w_got(w, 2, (2,))
        for half in (0, 1):
            for e in (1, -1):
                w_send(w, half, 2, 0, 1, e, (3, 2))

    def w_detour(half):
        at = (x, z)[half]
        p = w_piece(0, half, 0, -1, 0, 64 - DETOUR)
        send(way(half, 1, 1), p, p, ("w", 0, 4))
        turn = 1 - 2 * lax.rem(at, 2)
        other = lax.rem(at + turn + 4, 4)
        back = lax.rem(at - turn + 4, 4)
        start = (z * 4 + back if half == 0 else back * 4 + x) * 128 + half * 64 + 64 - DETOUR
        q = w_d.at[rows(start, DETOUR), :]
        send({"rep": z * 4 + other if half == 0 else other * 4 + x}, q, q, ("w", 0, 4))

    def w_third(w, d1):
        w_got(w, 4, (3, d1))
        s = 1 if d1 in PLUS[w] else -1
        for half in (0, 1):
            if (w, d1) == (0, 0):
                w_detour(half)
            else:
                w_send(w, half, d1, -s, 1, s, (4,))

    def w_last(w):
        w_got(w, 8, (4,))

    def unit(w, half, da, db):
        dz, dx = (db, da) if half == 0 else (da, db)
        return parts[w].at[rows(chunk(dz, dx), 128), half * 512 : half * 512 + 512]

    def rs_way(half, second, s):
        return way(1 - half, second, s)

    def sign(w, db):
        return 1 if db % 4 in PLUS[w] else -1

    def rs_got(w, units, stage):
        got(parts[w].at[0 : 128 * units, 0:512], ("rs", w, *stage))

    def end1(w, half, db, s):
        return (lft1 if s > 0 else rgt1).at[w, half, db]

    def end2(w, half, s):
        if w == 1:
            return (lft_out if s > 0 else rgt_out).at[half]
        return (lft2 if s > 0 else rgt2).at[half]

    def far(w, half, db):
        send(rs_way(half, 0, sign(w, db)), unit(w, half, 2, db), fwd1.at[w, half, db], ("rs", w, 1, db))

    def rs_far(w, dz):
        far(w, 0, dz)
        if dz == 2:
            for db in (2, 1, 3, 0):
                far(w, 1, db)

    def rs_near(w, db):
        s = -sign(w, db)
        for half in (0, 1):
            send(rs_way(half, 0, s), unit(w, half, s, db), end1(w, half, db, s), ("rs", w, 2, db))

    def rs_relay(w, db):
        s = sign(w, db)
        rs_got(w, 2, (1, db))
        for half in (0, 1):
            mine = unit(w, half, s, db)
            add(mine, mine, fwd1.at[w, half, db])
            send(rs_way(half, 0, s), mine, end1(w, half, db, s), ("rs", w, 2, db))

    def outs(w, half):
        return (gd_out, gu_out)[w].at[:, half * 512 : half * 512 + 512]

    def rs_mid(w, db):
        s = TURN[w]
        rs_got(w, 6 if db == s % 4 else 4, (2, db))
        for half in (0, 1):
            terms = [unit(w, half, 0, db), lft1.at[w, half, db], rgt1.at[w, half, db]]
            mine = sum1.at[w, half, db]
            if db == 2:
                add(mine, *terms)
                send(rs_way(half, 1, s), mine, fwd2.at[w, half], ("rs", w, 2, s % 4))
            elif db == -s % 4:
                add(mine, *terms)
                send(rs_way(half, 1, -s), mine, end2(w, half, -s), ("rs", w, 4))
            elif db == s % 4:
                add(mine, *terms, fwd2.at[w, half])
                send(rs_way(half, 1, s), mine, end2(w, half, s), ("rs", w, 4))
            else:
                add(outs(w, half), *terms)
        if db == 0:
            rs_got(w, 4, (4,))
            for half in (0, 1):
                if w == 0:
                    add(outs(w, half), outs(w, half), lft2.at[half], rgt2.at[half], scale=factor)

    def block(df, mine):
        core = tp if mine else 1 - tp
        return (ring(fs, df) * 2 + core) * 128

    def gi_rows(df, h):
        return part_i.at[rows(block(df, True) + h * 64, 64), :]

    def gi_pair():
        for df in (2, 1, 3, 0):
            src = part_i.at[rows(block(df, False), 128), :]
            send("co", src, pair_in.at[df], ("gi", 0, "pair"))

    def gi_got(pieces, stage):
        got(part_i.at[0 : 64 * pieces, :], ("gi", 0, stage))

    def gi_sum(df):
        mine = part_i.at[rows(block(df, True), 128), :]
        add(mine, mine, pair_in.at[df], size=16)

    def gi_far():
        gi_got(8, "pair")
        gi_sum(2)
        send("yp", gi_rows(2, 0), hop_f.at[0], ("gi", 0, "far"))
        send("ym", gi_rows(2, 1), hop_f.at[1], ("gi", 0, "far"))
        gi_sum(1)
        send("yp", gi_rows(1, 1), hop_l.at[1], ("gi", 0, "end"))
        gi_sum(3)
        send("ym", gi_rows(3, 0), hop_r.at[0], ("gi", 0, "end"))

    def gi_relay():
        gi_got(2, "far")
        add(gi_rows(1, 0), gi_rows(1, 0), hop_f.at[0], size=16)
        send("yp", gi_rows(1, 0), hop_l.at[0], ("gi", 0, "end"))
        add(gi_rows(3, 1), gi_rows(3, 1), hop_f.at[1], size=16)
        send("ym", gi_rows(3, 1), hop_r.at[1], ("gi", 0, "end"))

    def gi_end():
        gi_got(4, "end")
        for h in (0, 1):
            add(
                gi_out.at[pl.ds(h * 64, 64), :],
                gi_rows(0, h), pair_in.at[0, pl.ds(h * 64, 64), :], hop_l.at[h], hop_r.at[h], size=16,
            )

    def squares():
        here(1408, 1)

        def one(i, carry):
            r = rows(i * 32, 32)
            linear = jnp.maximum(pre[r, :].astype(F32), 0.0)
            sq[r, :] = (linear * linear).astype(BF16)
            return carry

        lax.fori_loop(0, 32, one, 0)

    def grad_tile(w, dz):
        right = (sq, gp)[w]
        start = ring(z, dz) * 512
        turned[...] = tokens[w][:, rows(start, 512)].T

        def one(j, carry):
            c = rows(j * 512, 512)
            parts[w][rows(start, 512), c] = jnp.dot(
                turned[...], right[:, c], preferred_element_type=F32
            ).astype(BF16)
            return carry

        lax.fori_loop(0, 2, one, 0)

    def pre_tile(i, half):
        def one(j, carry):
            r, c = rows(i * 512, 512), rows(half * 512 + j * 256, 256)
            acc = jnp.dot(tok_g[r, :], w_d[:, c], preferred_element_type=F32)
            linear = jnp.maximum(pre[r, c].astype(F32), 0.0)
            gp[r, c] = (acc * 2.0 * linear).astype(BF16)
            return carry

        lax.fori_loop(0, 2, one, 0)

    def term_tile(i, half):
        def one(j, carry):
            r, c = rows(i * 512, 512), rows(half * 1024 + j * 512, 512)
            part_i[r, c] = lax.dot_general(
                gp[r, :], w_u[c, :], (((1,), (1,)), ((), ())), preferred_element_type=F32
            ).astype(BF16)
            return carry

        lax.fori_loop(0, 2, one, 0)

    own = rows((fs * 2 + tp) * 128, 128)
    mine = rows(rep * 128, 128)
    local = [
        pltpu.make_async_copy(src, dst, local_sem.at[n // 2 if n < 4 else 1])
        for n, (src, dst) in enumerate(
            (
                (wd_in, w_d.at[mine, :]),
                (og, tok_g.at[own, :]),
                (wu_in, w_u.at[mine, :]),
                (inp, tok_x.at[own, :]),
                (pre_in, pre),
            )
        )
    ]
    for copy in local[:2]:
        copy.start()
    barrier = pltpu.get_barrier_semaphore()
    for name, to in target.items():
        to = to if name == "co" else {**to, "tp": 0 if name[0] == "z" else 1}
        pl.semaphore_signal(barrier, inc=1, device_id=to, device_id_type=MESH)

    def gather():
        pl.semaphore_wait(barrier, 5 + 4 * tp)
        pl.semaphore_signal(ready_sem, inc=1, device_id=target["co"], device_id_type=MESH)

    def hear():
        pl.semaphore_wait(ready_sem, 1)

    def along_z():
        w_own_along("z")

    def along_xy():
        w_own_along("x")
        tok_own(0)

    def begin():
        here(384, 0)
        later = lax.div(z + 3, 4)
        pl.when(tp + later == 1)(gather)
        pl.when(tp + later != 1)(hear)
        pl.when(later == 1)(along_z)
        pl.when(later == 0)(along_xy)
        pl.when(tp + later == 1)(hear)
        pl.when(tp + later != 1)(gather)
        pl.when(later == 1)(along_xy)
        pl.when(later == 0)(along_z)
        for copy in local[2:]:
            copy.start()

    def finish():
        sent(mats.at[:, 0:1920, :], "w")
        sent(toks.at[:, 0:896, :], "tok")
        sent(sums.at[:, 0:1920, :], "rs")
        sent(part_i.at[0:896, :], "gi")

    events = {f.__name__: f for f in (
        begin, squares, w_own, w_first, w_second, w_third, w_last, tok_own, tok_first, tok_second, tok_third, tok_partner,
        grad_tile, rs_far, rs_near, rs_relay, rs_mid, pre_tile, term_tile, gi_pair, gi_far, gi_relay, gi_end, finish,
    )}
    for n, (what, *args) in enumerate(PLAN):
        with jax.named_scope(":".join(str(v) for v in (what, *args)) + f"#n={n}"):
            events[what](*args)


def hand_over(gi_in, gu_in, gd_in, lft_in, rgt_in, gi_out, gu_out, gd_out, done, sem):
    copies = [
        pltpu.make_async_copy(src, dst, sem.at[n])
        for n, (src, dst) in enumerate(((gi_in, gi_out), (gd_in, gd_out)))
    ]
    for copy in copies:
        copy.start()
    for part in (0, 1):

        def one(i, carry, part=part):
            r = pl.ds(pl.multiple_of(part * 64 + i * 16, 16), 16)
            for half in (0, 1):
                c = slice(half * 512, half * 512 + 512)
                total = gu_in[r, c] + lft_in[half, r, :].astype(F32) + rgt_in[half, r, :].astype(F32)
                done[r, c] = total * FACTOR
            return carry

        lax.fori_loop(0, 4, one, 0)
        r = pl.ds(part * 64, 64)
        copies.append(pltpu.make_async_copy(done.at[r, :], gu_out.at[r, :], sem.at[2 + part]))
        copies[-1].start()
    for copy in copies:
        copy.wait()


def on_device(inputs, out_grad, pre_act, w_up, w_down_t):
    hbm = pl.BlockSpec(memory_space=pltpu.HBM)
    vmem = pl.BlockSpec(memory_space=pltpu.VMEM)
    outs = (
        jax.ShapeDtypeStruct((128, 2048), BF16),
        jax.ShapeDtypeStruct((128, 1024), F32),
        jax.ShapeDtypeStruct((128, 1024), F32),
    )

    def vm(*shape, kind=BF16):
        return pltpu.VMEM(shape, kind)

    results = pl.pallas_call(
        kernel,
        out_shape=(*outs, *[jax.ShapeDtypeStruct((2, 128, 512), BF16)] * 2),
        in_specs=[hbm] * 5,
        out_specs=(vmem,) * 5,
        scratch_shapes=[
            vm(2, 1024, 2048), vm(2, 2048, 1024),
            vm(1024, 1024), vm(1024, 1024), vm(1024, 1024), vm(512, 1024),
            vm(2, 2048, 1024), vm(1024, 2048),
            vm(2, 2, 4, 128, 512), vm(2, 2, 4, 128, 512), vm(2, 2, 4, 128, 512), vm(2, 2, 4, 128, 512),
            vm(2, 2, 128, 512), vm(2, 128, 512), vm(2, 128, 512),
            vm(4, 128, 2048), vm(2, 64, 2048), vm(2, 64, 2048), vm(2, 64, 2048),
            pltpu.SemaphoreType.DMA((4,)), pltpu.SemaphoreType.DMA((45,)), pltpu.SemaphoreType.DMA((2,)),
            pltpu.SemaphoreType.REGULAR,
        ],
        compiler_params=pltpu.CompilerParams(
            collective_id=0, has_side_effects=True, vmem_limit_bytes=54_000_000
        ),
        name="backward",
    )(*(pltpu.with_memory_space_constraint(v, pltpu.HBM) for v in (inputs, out_grad, pre_act, w_up, w_down_t)))
    return pl.pallas_call(
        hand_over,
        out_shape=outs,
        in_specs=[vmem] * 5,
        out_specs=(hbm,) * 3,
        scratch_shapes=[vm(128, 1024, kind=F32), pltpu.SemaphoreType.DMA((4,))],
        compiler_params=pltpu.CompilerParams(vmem_limit_bytes=4_000_000),
        name="hand_over",
    )(*results)


def solution(mesh):
    rows_all = P(("rep", "fs", "tp"), None)
    tiles = P("rep", ("fs", "tp"))
    return jax.shard_map(
        on_device,
        mesh=mesh,
        in_specs=(rows_all, rows_all, tiles, tiles, tiles),
        out_specs=(rows_all, tiles, tiles),
        check_vma=False,
    )
```

```python
import jax
import jax.numpy as jnp
from jax import lax
from jax.experimental import pallas as pl
from jax.experimental.pallas import tpu as pltpu
from jax.sharding import PartitionSpec as P

MESH = pl.DeviceIdType.MESH
BF16, F32 = jnp.bfloat16, jnp.float32
STEP = {"zp": (1, 0), "zm": (-1, 0), "xp": (0, 1), "xm": (0, -1)}
PLUS = ((0, 2), (1, 3))
TURN = (1, -1)
DETOUR = 16
FACTOR = 1.0 / 128.0
PLAN = (
    ("begin",), ("squares",), ("w_own", 1), ("w_first", 0, 1), ("w_first", 1, -1), ("w_first", 0, -1),
    ("tok_first", 0), ("w_second", 0), ("tok_own", 1), ("tok_third", 0), ("tok_second", 0), ("w_first", 1, 1),
    ("w_third", 0, 0), ("tok_partner", 0), ("w_second", 1), ("grad_tile", 0, 2), ("grad_tile", 0, 0),
    ("grad_tile", 0, 1), ("w_third", 0, 3), ("w_third", 0, 1), ("w_third", 0, 2), ("rs_far", 0, 2),
    ("tok_first", 1), ("grad_tile", 0, 3), ("w_third", 1, 1), ("w_third", 1, 0), ("w_third", 1, 2),
    ("w_last", 0), ("rs_far", 0, 3), ("w_third", 1, 3), ("tok_third", 1), ("rs_near", 0, 3),
    ("rs_near", 0, 1), ("pre_tile", 1, 0), ("rs_relay", 0, 2), ("rs_near", 0, 2), ("rs_far", 0, 1),
    ("tok_second", 1), ("pre_tile", 0, 1), ("tok_partner", 1), ("pre_tile", 0, 0), ("pre_tile", 1, 1),
    ("rs_relay", 0, 3), ("grad_tile", 1, 2), ("rs_far", 0, 0), ("grad_tile", 1, 1), ("rs_far", 1, 2),
    ("grad_tile", 1, 3), ("rs_relay", 0, 1), ("rs_far", 1, 3), ("rs_far", 1, 1), ("rs_near", 1, 3),
    ("rs_near", 1, 2), ("w_last", 1), ("term_tile", 1, 1), ("term_tile", 0, 0), ("term_tile", 1, 0),
    ("term_tile", 0, 1), ("rs_mid", 0, 2), ("rs_relay", 1, 2), ("gi_pair",), ("rs_near", 0, 0),
    ("rs_relay", 0, 0), ("rs_relay", 1, 1), ("gi_far",), ("rs_near", 1, 1), ("grad_tile", 1, 0),
    ("rs_far", 1, 0), ("rs_mid", 1, 2), ("rs_relay", 1, 3), ("rs_mid", 0, 1), ("rs_near", 1, 0),
    ("gi_relay",), ("rs_mid", 0, 3), ("rs_mid", 1, 1), ("rs_relay", 1, 0), ("rs_mid", 1, 3), ("rs_mid", 0, 0),
    ("gi_end",), ("rs_mid", 1, 0), ("finish",),
)


def kernel(
    inp, og, pre_in, wu_in, wd_in, gi_out, gu_out, gd_out, lft_out, rgt_out,
    toks, mats, pre, sq, gp, turned, sums, part_i,
    fwd1, lft1, rgt1, sum1, fwd2, lft2, rgt2,
    pair_in, hop_f, hop_l, hop_r, send_sem, recv_sem, local_sem, ready_sem,
):
    rep, fs, tp = lax.axis_index("rep"), lax.axis_index("fs"), lax.axis_index("tp")
    z, x = lax.div(rep, 4), lax.rem(rep, 4)
    tokens, weights, parts = [[ref.at[0], ref.at[1]] for ref in (toks, mats, sums)]
    (tok_g, tok_x), (w_d, w_u) = tokens, weights
    factor = FACTOR

    def ring(v, d):
        return lax.rem(v + d % 4, 4)

    target = {
        "zp": {"rep": ring(z, 1) * 4 + x},
        "zm": {"rep": ring(z, -1) * 4 + x},
        "xp": {"rep": z * 4 + ring(x, 1)},
        "xm": {"rep": z * 4 + ring(x, -1)},
        "yp": {"fs": ring(fs, 1)},
        "ym": {"fs": ring(fs, -1)},
        "co": {"tp": 1 - tp},
    }
    groups, classes = {}, {}

    def remote(to, src, dst, group, kind):
        k = classes.setdefault(kind, len(classes))
        n = groups.setdefault(group, len(groups))
        return pltpu.make_async_remote_copy(
            src_ref=src, dst_ref=dst, send_sem=send_sem.at[k], recv_sem=recv_sem.at[n],
            device_id=target[to] if isinstance(to, str) else to, device_id_type=MESH,
        )

    def send(to, src, dst, group):
        remote(to, src, dst, group, group[0]).start()

    def got(like, group):
        remote("co", like, like, group, group[0]).wait_recv()

    def here(count, n):
        like = w_u.at[0:count, :]
        pltpu.make_async_copy(like, like, local_sem.at[n]).wait()

    def sent(like, kind):
        remote("co", like, like, ("w", 0, 4), kind).wait_send()

    def rows(start, size):
        return pl.ds(pl.multiple_of(start, size & -size), size)

    def add(dst, *srcs, size=32, scale=None):
        def one(i, carry):
            r = rows(i * size, size)
            total = srcs[0][r, :].astype(F32)
            for src in srcs[1:]:
                total = total + src[r, :].astype(F32)
            if scale is not None:
                total = total * scale
            dst[r, :] = total.astype(dst.dtype)
            return carry

        lax.fori_loop(0, dst.shape[0] // size, one, 0)

    def tok(a, df, mine, h):
        core = tp if mine else 1 - tp
        return tokens[a].at[rows((ring(fs, df) * 2 + core) * 128 + h * 64, 64), :]

    def tok_y(a, df, h, s, stage):
        p = tok(a, df, True, h)
        send("yp" if s > 0 else "ym", p, p, ("tok", a, stage))

    def tok_co(a, df, h):
        p = tok(a, df, True, h)
        send("co", p, p, ("tok", a, "partner"))

    def tok_got(a, pieces, stage):
        got(tokens[a].at[0 : 64 * pieces, :], ("tok", a, stage))

    def tok_own(a):
        tok_y(a, 0, 0, 1, 1)
        tok_y(a, 0, 1, -1, 1)
        tok_y(a, 0, 1, 1, 2)
        tok_y(a, 0, 0, -1, 2)
        tok_co(a, 0, 0)
        tok_co(a, 0, 1)

    def tok_first(a):
        tok_got(a, 2, 1)
        for df, h in ((-1, 0), (1, 1)):
            tok_y(a, df, h, -df, 3)
            tok_co(a, df, h)

    def tok_second(a):
        tok_got(a, 2, 2)
        for df, h in ((-1, 1), (1, 0)):
            tok_co(a, df, h)

    def tok_third(a):
        tok_got(a, 2, 3)
        for h in (0, 1):
            tok_co(a, 2, h)

    def tok_partner(a):
        tok_got(a, 8, "partner")

    def chunk(dz, dx):
        return (ring(z, dz) * 4 + ring(x, dx)) * 128

    def offs(half, d1, d2):
        return (d1, d2) if half == 0 else (d2, d1)

    def way(half, second, s):
        return ("zx"[half ^ second]) + ("p" if s > 0 else "m")

    def w_piece(w, half, d1, d2, off=0, size=64):
        dz, dx = offs(half, d1, d2)
        return weights[w].at[rows(chunk(dz, dx) + half * 64 + off, size), :]

    def w_send(w, half, d1, d2, second, s, stage):
        p = w_piece(w, half, d1, d2)
        send(way(half, second, s), p, p, ("w", w, *stage))

    def w_got(w, pieces, stage):
        got(weights[w].at[0 : 64 * pieces, :], ("w", w, *stage))

    def w_own(w):
        for second in (0, 1):
            for half in (0, 1):
                for s in (1, -1):
                    w_send(w, half, 0, 0, second, s, (3, 0) if second else (1, s))

    def w_own_along(axis):
        for second in (0, 1):
            half = second if axis == "z" else 1 - second
            for s in (1, -1):
                w_send(0, half, 0, 0, second, s, (3, 0) if second else (1, s))

    def w_first(w, s):
        w_got(w, 2, (1, s))
        if s == TURN[w]:
            for half in (0, 1):
                w_send(w, half, -s, 0, 0, s, (2,))
        for half in (0, 1):
            for e in (1, -1):
                w_send(w, half, -s, 0, 1, e, (3, -s % 4))

    def w_second(w):
        w_got(w, 2, (2,))
        for half in (0, 1):
            for e in (1, -1):
                w_send(w, half, 2, 0, 1, e, (3, 2))

    def w_detour(half):
        at = (x, z)[half]
        p = w_piece(0, half, 0, -1, 0, 64 - DETOUR)
        send(way(half, 1, 1), p, p, ("w", 0, 4))
        turn = 1 - 2 * lax.rem(at, 2)
        other = lax.rem(at + turn + 4, 4)
        back = lax.rem(at - turn + 4, 4)
        start = (z * 4 + back if half == 0 else back * 4 + x) * 128 + half * 64 + 64 - DETOUR
        q = w_d.at[rows(start, DETOUR), :]
        send({"rep": z * 4 + other if half == 0 else other * 4 + x}, q, q, ("w", 0, 4))

    def w_third(w, d1):
        w_got(w, 4, (3, d1))
        s = 1 if d1 in PLUS[w] else -1
        for half in (0, 1):
            if (w, d1) == (0, 0):
                w_detour(half)
            else:
                w_send(w, half, d1, -s, 1, s, (4,))

    def w_last(w):
        w_got(w, 8, (4,))

    def unit(w, half, da, db):
        dz, dx = (db, da) if half == 0 else (da, db)
        return parts[w].at[rows(chunk(dz, dx), 128), half * 512 : half * 512 + 512]

    def rs_way(half, second, s):
        return way(1 - half, second, s)

    def sign(w, db):
        return 1 if db % 4 in PLUS[w] else -1

    def rs_got(w, units, stage):
        got(parts[w].at[0 : 128 * units, 0:512], ("rs", w, *stage))

    def end1(w, half, db, s):
        return (lft1 if s > 0 else rgt1).at[w, half, db]

    def end2(w, half, s):
        if w == 1:
            return (lft_out if s > 0 else rgt_out).at[half]
        return (lft2 if s > 0 else rgt2).at[half]

    def far(w, half, db):
        send(rs_way(half, 0, sign(w, db)), unit(w, half, 2, db), fwd1.at[w, half, db], ("rs", w, 1, db))

    def rs_far(w, dz):
        far(w, 0, dz)
        if dz == 2:
            for db in (2, 1, 3, 0):
                far(w, 1, db)

    def rs_near(w, db):
        s = -sign(w, db)
        for half in (0, 1):
            send(rs_way(half, 0, s), unit(w, half, s, db), end1(w, half, db, s), ("rs", w, 2, db))

    def rs_relay(w, db):
        s = sign(w, db)
        rs_got(w, 2, (1, db))
        for half in (0, 1):
            mine = unit(w, half, s, db)
            add(mine, mine, fwd1.at[w, half, db])
            send(rs_way(half, 0, s), mine, end1(w, half, db, s), ("rs", w, 2, db))

    def outs(w, half):
        return (gd_out, gu_out)[w].at[:, half * 512 : half * 512 + 512]

    def rs_mid(w, db):
        s = TURN[w]
        rs_got(w, 6 if db == s % 4 else 4, (2, db))
        for half in (0, 1):
            terms = [unit(w, half, 0, db), lft1.at[w, half, db], rgt1.at[w, half, db]]
            mine = sum1.at[w, half, db]
            if db == 2:
                add(mine, *terms)
                send(rs_way(half, 1, s), mine, fwd2.at[w, half], ("rs", w, 2, s % 4))
            elif db == -s % 4:
                add(mine, *terms)
                send(rs_way(half, 1, -s), mine, end2(w, half, -s), ("rs", w, 4))
            elif db == s % 4:
                add(mine, *terms, fwd2.at[w, half])
                send(rs_way(half, 1, s), mine, end2(w, half, s), ("rs", w, 4))
            else:
                add(outs(w, half), *terms)
        if db == 0:
            rs_got(w, 4, (4,))
            for half in (0, 1):
                if w == 0:
                    add(outs(w, half), outs(w, half), lft2.at[half], rgt2.at[half], scale=factor)

    def block(df, mine):
        core = tp if mine else 1 - tp
        return (ring(fs, df) * 2 + core) * 128

    def gi_rows(df, h):
        return part_i.at[rows(block(df, True) + h * 64, 64), :]

    def gi_pair():
        for df in (2, 1, 3, 0):
            src = part_i.at[rows(block(df, False), 128), :]
            send("co", src, pair_in.at[df], ("gi", 0, "pair"))

    def gi_got(pieces, stage):
        got(part_i.at[0 : 64 * pieces, :], ("gi", 0, stage))

    def gi_sum(df):
        mine = part_i.at[rows(block(df, True), 128), :]
        add(mine, mine, pair_in.at[df], size=16)

    def gi_far():
        gi_got(8, "pair")
        gi_sum(2)
        send("yp", gi_rows(2, 0), hop_f.at[0], ("gi", 0, "far"))
        send("ym", gi_rows(2, 1), hop_f.at[1], ("gi", 0, "far"))
        gi_sum(1)
        send("yp", gi_rows(1, 1), hop_l.at[1], ("gi", 0, "end"))
        gi_sum(3)
        send("ym", gi_rows(3, 0), hop_r.at[0], ("gi", 0, "end"))

    def gi_relay():
        gi_got(2, "far")
        add(gi_rows(1, 0), gi_rows(1, 0), hop_f.at[0], size=16)
        send("yp", gi_rows(1, 0), hop_l.at[0], ("gi", 0, "end"))
        add(gi_rows(3, 1), gi_rows(3, 1), hop_f.at[1], size=16)
        send("ym", gi_rows(3, 1), hop_r.at[1], ("gi", 0, "end"))

    def gi_end():
        gi_got(4, "end")
        for h in (0, 1):
            add(
                gi_out.at[pl.ds(h * 64, 64), :],
                gi_rows(0, h), pair_in.at[0, pl.ds(h * 64, 64), :], hop_l.at[h], hop_r.at[h], size=16,
            )

    def squares():
        here(1408, 1)

        def one(i, carry):
            r = rows(i * 32, 32)
            linear = jnp.maximum(pre[r, :].astype(F32), 0.0)
            sq[r, :] = (linear * linear).astype(BF16)
            return carry

        lax.fori_loop(0, 32, one, 0)

    def grad_tile(w, dz):
        right = (sq, gp)[w]
        start = ring(z, dz) * 512
        turned[...] = tokens[w][:, rows(start, 512)].T

        def one(j, carry):
            c = rows(j * 512, 512)
            parts[w][rows(start, 512), c] = jnp.dot(
                turned[...], right[:, c], preferred_element_type=F32
            ).astype(BF16)
            return carry

        lax.fori_loop(0, 2, one, 0)

    def pre_tile(i, half):
        def one(j, carry):
            r, c = rows(i * 512, 512), rows(half * 512 + j * 256, 256)
            acc = jnp.dot(tok_g[r, :], w_d[:, c], preferred_element_type=F32)
            linear = jnp.maximum(pre[r, c].astype(F32), 0.0)
            gp[r, c] = (acc * 2.0 * linear).astype(BF16)
            return carry

        lax.fori_loop(0, 2, one, 0)

    def term_tile(i, half):
        def one(j, carry):
            r, c = rows(i * 512, 512), rows(half * 1024 + j * 512, 512)
            part_i[r, c] = lax.dot_general(
                gp[r, :], w_u[c, :], (((1,), (1,)), ((), ())), preferred_element_type=F32
            ).astype(BF16)
            return carry

        lax.fori_loop(0, 2, one, 0)

    own = rows((fs * 2 + tp) * 128, 128)
    mine = rows(rep * 128, 128)
    local = [
        pltpu.make_async_copy(src, dst, local_sem.at[n // 2 if n < 4 else 1])
        for n, (src, dst) in enumerate(
            (
                (wd_in, w_d.at[mine, :]),
                (og, tok_g.at[own, :]),
                (wu_in, w_u.at[mine, :]),
                (inp, tok_x.at[own, :]),
                (pre_in, pre),
            )
        )
    ]
    for copy in local[:2]:
        copy.start()
    later = lax.div(z + 3, 4)
    barrier = pltpu.get_barrier_semaphore()
    for name, to in target.items():
        to = to if name == "co" else {**to, "tp": {"z": 0, "x": 1, "y": later}[name[0]]}
        pl.semaphore_signal(barrier, inc=1, device_id=to, device_id_type=MESH)

    def gather():
        pl.semaphore_wait(barrier, 9 - 4 * (tp - later) * (tp - later))
        pl.semaphore_signal(ready_sem, inc=1, device_id=target["co"], device_id_type=MESH)

    def hear():
        pl.semaphore_wait(ready_sem, 1)

    def along_z():
        w_own_along("z")

    def along_x():
        w_own_along("x")

    def begin():
        here(384, 0)
        pl.when(tp + later == 1)(gather)
        pl.when(tp + later != 1)(hear)
        pl.when(later == 1)(along_z)
        pl.when(later == 0)(along_x)
        pl.when(tp + later == 1)(hear)
        pl.when(tp + later != 1)(gather)
        pl.when(later == 1)(along_x)
        pl.when(later == 0)(along_z)
        tok_own(0)
        for copy in local[2:]:
            copy.start()

    def finish():
        sent(mats.at[:, 0:1920, :], "w")
        sent(toks.at[:, 0:896, :], "tok")
        sent(sums.at[:, 0:1920, :], "rs")
        sent(part_i.at[0:896, :], "gi")

    events = {f.__name__: f for f in (
        begin, squares, w_own, w_first, w_second, w_third, w_last, tok_own, tok_first, tok_second, tok_third, tok_partner,
        grad_tile, rs_far, rs_near, rs_relay, rs_mid, pre_tile, term_tile, gi_pair, gi_far, gi_relay, gi_end, finish,
    )}
    for n, (what, *args) in enumerate(PLAN):
        with jax.named_scope(":".join(str(v) for v in (what, *args)) + f"#n={n}"):
            events[what](*args)


def hand_over(gi_in, gu_in, gd_in, lft_in, rgt_in, gi_out, gu_out, gd_out, done, sem):
    copies = [
        pltpu.make_async_copy(src, dst, sem.at[n])
        for n, (src, dst) in enumerate(((gi_in, gi_out), (gd_in, gd_out)))
    ]
    for copy in copies:
        copy.start()
    for part in (0, 1):

        def one(i, carry, part=part):
            r = pl.ds(pl.multiple_of(part * 64 + i * 16, 16), 16)
            for half in (0, 1):
                c = slice(half * 512, half * 512 + 512)
                total = gu_in[r, c] + lft_in[half, r, :].astype(F32) + rgt_in[half, r, :].astype(F32)
                done[r, c] = total * FACTOR
            return carry

        lax.fori_loop(0, 4, one, 0)
        r = pl.ds(part * 64, 64)
        copies.append(pltpu.make_async_copy(done.at[r, :], gu_out.at[r, :], sem.at[2 + part]))
        copies[-1].start()
    for copy in copies:
        copy.wait()


def on_device(inputs, out_grad, pre_act, w_up, w_down_t):
    hbm = pl.BlockSpec(memory_space=pltpu.HBM)
    vmem = pl.BlockSpec(memory_space=pltpu.VMEM)
    outs = (
        jax.ShapeDtypeStruct((128, 2048), BF16),
        jax.ShapeDtypeStruct((128, 1024), F32),
        jax.ShapeDtypeStruct((128, 1024), F32),
    )

    def vm(*shape, kind=BF16):
        return pltpu.VMEM(shape, kind)

    results = pl.pallas_call(
        kernel,
        out_shape=(*outs, *[jax.ShapeDtypeStruct((2, 128, 512), BF16)] * 2),
        in_specs=[hbm] * 5,
        out_specs=(vmem,) * 5,
        scratch_shapes=[
            vm(2, 1024, 2048), vm(2, 2048, 1024),
            vm(1024, 1024), vm(1024, 1024), vm(1024, 1024), vm(512, 1024),
            vm(2, 2048, 1024), vm(1024, 2048),
            vm(2, 2, 4, 128, 512), vm(2, 2, 4, 128, 512), vm(2, 2, 4, 128, 512), vm(2, 2, 4, 128, 512),
            vm(2, 2, 128, 512), vm(2, 128, 512), vm(2, 128, 512),
            vm(4, 128, 2048), vm(2, 64, 2048), vm(2, 64, 2048), vm(2, 64, 2048),
            pltpu.SemaphoreType.DMA((4,)), pltpu.SemaphoreType.DMA((45,)), pltpu.SemaphoreType.DMA((2,)),
            pltpu.SemaphoreType.REGULAR,
        ],
        compiler_params=pltpu.CompilerParams(
            collective_id=0, has_side_effects=True, vmem_limit_bytes=54_000_000
        ),
        name="backward",
    )(*(pltpu.with_memory_space_constraint(v, pltpu.HBM) for v in (inputs, out_grad, pre_act, w_up, w_down_t)))
    return pl.pallas_call(
        hand_over,
        out_shape=outs,
        in_specs=[vmem] * 5,
        out_specs=(hbm,) * 3,
        scratch_shapes=[vm(128, 1024, kind=F32), pltpu.SemaphoreType.DMA((4,))],
        compiler_params=pltpu.CompilerParams(vmem_limit_bytes=4_000_000),
        name="hand_over",
    )(*results)


def solution(mesh):
    rows_all = P(("rep", "fs", "tp"), None)
    tiles = P("rep", ("fs", "tp"))
    return jax.shard_map(
        on_device,
        mesh=mesh,
        in_specs=(rows_all, rows_all, tiles, tiles, tiles),
        out_specs=(rows_all, tiles, tiles),
        check_vma=False,
    )
```
